32 devices in a mesh: sp: 8 (over z, x), tp: 4 (over y, core).
Axes of the slice: x: 2, y: 2, z: 4, core: 2. Of those that a mesh axis runs over, the one named last changes fastest.
Arguments:
- prompt_tokens: bfloat16 [8192, 2048], P(('sp', 'tp')), may hold values from -8 to 8
- key_weight: bfloat16 [2048, 2048], P(None, 'tp'), may hold values from -0.125 to 0.125
- value_weight: bfloat16 [2048, 4096], P(None, 'tp'), may hold values from -0.125 to 0.125
- input_weight: bfloat16 [2048, 32], replicated, may hold values from -4 to 4
- forget_weight: bfloat16 [2048, 32], replicated, may hold values from -0.125 to 0.125
- forget_bias: float32 [32], replicated, as said below
- new_token: bfloat16 [2048], replicated, may hold values from -8 to 8
- new_query: bfloat16 [2048], P('tp'), may hold values from -6 to 6
Outputs:
- key_cache: bfloat16 [8192, 2048], P('sp', 'tp')
- value_cache: bfloat16 [8192, 4096], P('sp', 'tp')
- cache_weight: float32 [32, 8192], P('tp', 'sp')
- reading: float32 [4096], P('tp')
The draws below stay inside these ranges and needn't reach their ends.
Inputs may be any that keep to these rules, and one draw needn't show every extreme that they name: `forget_bias`: every head's forget gate offset is 2 or more.
All inputs are finite; a program needn't handle non-finite values.
Results may differ from the reference program's by a relative error of at most 0.0058.
Values may be sent and summed in bfloat16 or wider, within the bound.
No kernel may reach another device: no remote copies, remote signals or barrier semaphores. Data moves between devices by JAX's collectives and lax.ppermute only.
A program may use at most 64 MiB of HBM per device.

```python
import math
import jax
import jax.numpy as jnp
from jax import lax

D = 2048
H = 32
DQK = 64
DV = 128
LEN = 8192


def draw_prompt_tokens(key, part):
    base_key = jax.random.fold_in(key, 11)
    scale_key = jax.random.fold_in(key, 12)
    base_draw = jnp.clip(jax.random.normal(base_key, (LEN, D), jnp.float32), -5.0, 5.0)
    block_count = LEN // 32
    block_scales = jnp.exp(jax.random.uniform(scale_key, (block_count, 1), jnp.float32, math.log(0.5), math.log(1.6)))
    block_scales = jnp.repeat(block_scales, 32, axis=0)
    return (base_draw * block_scales).astype(jnp.bfloat16)


def draw_input_weight(key, part):
    base_draw = jnp.clip(jax.random.normal(jax.random.fold_in(key, 21), (D, H), jnp.float32), -4.0, 4.0) * D ** (-0.5)
    return base_draw.astype(jnp.bfloat16)


def draw_forget_bias(key, part):
    picked = jax.random.uniform(jax.random.fold_in(key, 31), (H,), jnp.float32)
    quick_rates = jax.random.uniform(jax.random.fold_in(key, 32), (H,), jnp.float32, 3.0, 4.5)
    slow_rates = math.log(LEN) + jax.random.uniform(jax.random.fold_in(key, 33), (H,), jnp.float32, 0.0, 1.5)
    quick_share = 0.5
    return jnp.where(picked < quick_share, quick_rates, slow_rates)


def level_of(key, dims, split, low, largest):
    factor_of, own = 1.0, jax.random.fold_in(key, 6)
    for axis_at, shards_of in split:
        steps = jnp.exp(jax.random.uniform(jax.random.fold_in(own, axis_at), (shards_of,), jnp.float32, low / len(split), largest / len(split)))
        factor_of = factor_of * jnp.repeat(steps, dims[axis_at] // shards_of).reshape([-1 if axis == axis_at else 1 for axis in range(len(dims))])
    return factor_of


def centred(own_key, extent, spread, limit, pieces=(), kind=jnp.bfloat16):
    factor_of = level_of(own_key, extent, pieces, -0.22, 0.18) if pieces else 1.0
    drawn = jax.random.normal(own_key, extent, jnp.float32) * spread * factor_of
    return jnp.minimum(jnp.maximum(drawn, -limit), limit).astype(kind)


def setup_inputs(seed: int = 0) -> dict:
    streams_of = jax.random.split(jax.random.key(seed), 9)
    prompt_tokens = draw_prompt_tokens(jax.random.fold_in(streams_of[8], 71), 0)
    key_weight = centred(streams_of[1], (D, H * DQK), D ** -0.5, 0.125, ((1, 4),))
    value_weight = centred(streams_of[2], (D, H * DV), D ** -0.5, 0.125, ((1, 4),))
    input_weight = draw_input_weight(jax.random.fold_in(streams_of[8], 71), 0)
    forget_weight = centred(streams_of[4], (D, H), D ** -0.5, 0.125)
    forget_bias = draw_forget_bias(jax.random.fold_in(streams_of[8], 71), 0)
    new_token = centred(streams_of[6], (D,), 2.0, 8.0)
    new_query = centred(streams_of[7], (H * DQK,), 1.0, 6.0, ((0, 4),))
    return {"prompt_tokens": prompt_tokens, "key_weight": key_weight, "value_weight": value_weight, "input_weight": input_weight, "forget_weight": forget_weight, "forget_bias": forget_bias, "new_token": new_token, "new_query": new_query}


def reference(prompt_tokens, key_weight, value_weight, input_weight, forget_weight, forget_bias, new_token, new_query):
    key_cache = jnp.dot(prompt_tokens, key_weight, preferred_element_type=jnp.float32).astype(jnp.bfloat16)
    value_cache = jnp.dot(prompt_tokens, value_weight, preferred_element_type=jnp.float32).astype(jnp.bfloat16)
    input_gate = jnp.dot(prompt_tokens, input_weight, preferred_element_type=jnp.float32)
    log_forget = jax.nn.log_sigmoid(jnp.dot(prompt_tokens, forget_weight, preferred_element_type=jnp.float32) + forget_bias)
    log_weight = input_gate + (lax.optimization_barrier(jnp.sum(log_forget, axis=0, keepdims=True)) - jnp.cumsum(log_forget, axis=0))
    peak_log = lax.optimization_barrier(jnp.max(log_weight, axis=0))
    cache_weight = jnp.transpose(jnp.exp(log_weight - peak_log[None, :]), (1, 0))
    new_key = jnp.dot(new_token, key_weight, preferred_element_type=jnp.float32).astype(jnp.bfloat16)
    new_value = jnp.dot(new_token, value_weight, preferred_element_type=jnp.float32).astype(jnp.bfloat16)
    new_gate = jnp.dot(new_token, input_weight, preferred_element_type=jnp.float32)
    new_forget = jax.nn.log_sigmoid(jnp.dot(new_token, forget_weight, preferred_element_type=jnp.float32) + forget_bias)
    stable_level = jnp.maximum(new_forget + peak_log, new_gate)
    query_heads = new_query.astype(jnp.float32).reshape(H, DQK)
    key_heads = key_cache.astype(jnp.float32).reshape(LEN, H, DQK)
    key_score = jnp.einsum('shd,hd->sh', key_heads, query_heads, precision=lax.Precision.HIGHEST) / math.sqrt(DQK)
    new_heads = new_key.astype(jnp.float32).reshape(H, DQK)
    new_score = jnp.einsum('hd,hd->h', new_heads, query_heads, precision=lax.Precision.HIGHEST) / math.sqrt(DQK)
    weighted = jnp.exp(new_forget[None, :] + log_weight - stable_level[None, :]) * key_score
    weighted_low = weighted.astype(jnp.bfloat16)
    own_term = jnp.exp(new_gate - stable_level) * new_score
    value_heads = value_cache.astype(jnp.float32).reshape(LEN, H, DV)
    numerator = jnp.einsum('sh,she->he', weighted_low.astype(jnp.float32), value_heads, precision=lax.Precision.HIGHEST)
    numerator = numerator + own_term[:, None] * new_value.astype(jnp.float32).reshape(H, DV)
    denominator = lax.optimization_barrier(jnp.sum(weighted, axis=0)) + own_term
    reading = numerator / jnp.maximum(jnp.abs(denominator), 1.0)[:, None]
    return (key_cache, value_cache, cache_weight, reading.reshape(H * DV))
```

```python
import functools
import math

import jax
import jax.numpy as jnp
from jax import lax
from jax.experimental import pallas as pl
from jax.experimental.pallas import tpu as pltpu
from jax.sharding import PartitionSpec as P

DQK = 64
DV = 128
LANES = 128
F32 = jnp.float32
BF16 = jnp.bfloat16

TOTAL, PEAK, DENOM, CARRIED = 0, 1, 2, 3
NEW_GATE, NEW_FORGET, NEW_SCORE = 4, 5, 6


def params(mib=24):
    return pltpu.CompilerParams(vmem_limit_bytes=mib * 1024 * 1024)


def cost(flops, moved):
    return pl.CostEstimate(flops=int(flops), bytes_accessed=int(moved), transcendentals=0)


def vmem():
    return pl.BlockSpec(memory_space=pltpu.VMEM)


def log_sigmoid(x):
    z = jnp.exp(-jnp.abs(x))
    u = 1.0 + z
    log1p = jnp.where(u == 1.0, z, jnp.log(u) * z / jnp.where(u == 1.0, 1.0, u - 1.0))
    return jnp.minimum(x, 0.0) - log1p


def split2(x):
    high = x.astype(BF16)
    return high, (x - high.astype(F32)).astype(BF16)


def lane_pack(values, rows):
    lane = lax.broadcasted_iota(jnp.int32, (rows, LANES), 1)
    out = jnp.zeros((rows, LANES), F32)
    for at, value in values.items():
        out = jnp.where(lane == at, value, out)
    return out


def nt_dot(a, b):
    return lax.dot_general(a, b, (((1,), (1,)), ((), ())), preferred_element_type=F32)


def fold_kernel(heads, first, query_ref, key_ref, x_ref, fold_ref, chunk_ref):
    width = query_ref.shape[1]
    owner = lax.broadcasted_iota(jnp.int32, (heads, width), 1) // DQK
    head = lax.broadcasted_iota(jnp.int32, (heads, width), 0)
    query = jnp.where(owner == head, query_ref[...].astype(F32), 0.0).astype(BF16)
    folded = nt_dot(query, key_ref[...])
    high, low = split2(folded)
    fold_ref[...] = jnp.concatenate([high, low], axis=0)
    chunk_ref[...] = x_ref[first : first + chunk_ref.shape[0], :]


def fold(query, key_weight, x, heads, first, rows):
    depth = key_weight.shape[0]
    return pl.pallas_call(
        functools.partial(fold_kernel, heads, first),
        out_shape=(
            jax.ShapeDtypeStruct((2 * heads, depth), BF16),
            jax.ShapeDtypeStruct((rows, depth), BF16),
        ),
        in_specs=[vmem(), vmem(), vmem()],
        out_specs=(vmem(), vmem()),
        compiler_params=params(),
        cost_estimate=cost(2e9, 3e6),
        name="fold",
    )(query, key_weight, x)


def local_kernel(heads, groups, spans, *refs):
    own_ref, other_ref, gate_ref, forget_ref, bias_ref, token_ref = refs[:6]
    fold_refs = refs[6 : 6 + groups]
    outs = refs[6 + groups + 1 :]
    message_refs, chunk_refs = outs[:groups], outs[groups : groups + len(spans)]
    left_ref, product_ref, weight_ref = outs[groups + len(spans) :]
    rows, depth = own_ref.shape
    every = gate_ref.shape[0]
    at = lax.axis_index("tp")
    core, chip = lax.rem(at, 2), at // 2
    for ref, (first, count) in zip(chunk_refs, spans, strict=True):
        ref[...] = own_ref[first : first + count, :]
    left_ref[0:every, :] = gate_ref[...]
    left_ref[every : 2 * every, :] = forget_ref[...]
    for g in range(groups):
        left_ref[2 * every + 2 * heads * g : 2 * every + 2 * heads * (g + 1), :] = fold_refs[g][...]
    left = left_ref[...]
    own_at = pl.multiple_of(core * rows, rows)
    other_at = pl.multiple_of((1 - core) * rows, rows)
    product_ref[:, pl.ds(own_at, rows)] = nt_dot(left, own_ref[...])
    product_ref[:, pl.ds(other_at, rows)] = nt_dot(left, other_ref[...])

    diagonal = lax.broadcasted_iota(jnp.int32, (every, every), 0) == lax.broadcasted_iota(
        jnp.int32, (every, every), 1
    )
    bias = jnp.sum(jnp.where(diagonal, bias_ref[...], 0.0), axis=1, keepdims=True)
    product_ref[every : 2 * every, :] = product_ref[every : 2 * every, :] + bias

    starts = [(lax.rem(chip + g, groups) * 2 + core) * heads for g in range(groups)]
    base = 2 * every

    def pick(of, first, start):
        out = of[first : first + heads, :]
        for k in range(heads, every, heads):
            out = jnp.where(start == k, of[first + k : first + k + heads, :], out)
        return out

    gates = jnp.concatenate([pick(product_ref, 0, s) for s in starts], axis=0)
    forgets = jnp.concatenate([pick(product_ref, every, s) for s in starts], axis=0)
    scores = jnp.concatenate(
        [
            product_ref[base + 2 * heads * g : base + 2 * heads * g + heads, :]
            + product_ref[base + 2 * heads * g + heads : base + 2 * heads * (g + 1), :]
            for g in range(groups)
        ],
        axis=0,
    ) * (1.0 / math.sqrt(DQK))
    total_rows = groups * heads
    log_forget = log_sigmoid(forgets)
    high = log_forget.astype(BF16)
    rest = log_forget - high.astype(F32)
    middle = rest.astype(BF16)
    low = (rest - middle.astype(F32)).astype(BF16)
    later = (
        lax.broadcasted_iota(jnp.int32, (rows, rows), 0)
        > lax.broadcasted_iota(jnp.int32, (rows, rows), 1)
    ).astype(F32).astype(BF16)

    def suffix(first):
        def part(v):
            return jnp.dot(v[:, first : first + rows], later, preferred_element_type=F32)

        return part(high) + (part(middle) + part(low))

    first_total = jnp.sum(log_forget[:, :rows], axis=1, keepdims=True)
    second_total = jnp.sum(log_forget[:, rows:], axis=1, keepdims=True)
    log_weight = gates + jnp.concatenate([suffix(0) + second_total, suffix(rows)], axis=1)
    peak = jnp.max(log_weight, axis=1, keepdims=True)
    weighted = jnp.exp(log_weight - peak) * scores
    denom = jnp.sum(weighted, axis=1, keepdims=True)
    total = first_total + second_total
    weight_ref[...] = weighted.astype(BF16)
    summed = jnp.dot(
        weight_ref[:, pl.ds(own_at, rows)], own_ref[...], preferred_element_type=F32
    ) + jnp.dot(weight_ref[:, pl.ds(other_at, rows)], other_ref[...], preferred_element_type=F32)

    token = token_ref[...].astype(F32)

    def of_token(rows_of):
        return jnp.sum(rows_of.astype(F32) * token, axis=1, keepdims=True)

    new_all = of_token(left_ref[0 : 2 * every, :])
    new_fold = of_token(left_ref[base : base + 2 * heads, :])
    new_gate = pick(new_all, 0, starts[0])
    new_forget = pick(log_sigmoid(new_all[every:] + bias), 0, starts[0])
    new_score = (new_fold[:heads] + new_fold[heads:]) * (1.0 / math.sqrt(DQK))

    for g in range(groups):
        mine = slice(g * heads, (g + 1) * heads)
        stats = {TOTAL: total[mine], PEAK: peak[mine], DENOM: denom[mine]}
        if g == 0:
            stats |= {NEW_GATE: new_gate, NEW_FORGET: new_forget, NEW_SCORE: new_score}
        message_refs[g][:, :depth] = summed[mine]
        message_refs[g][:, depth : depth + 2 * rows] = log_weight[mine]
        message_refs[g][:, depth + 2 * rows :] = lane_pack(stats, heads)


def local(own, other, gate_t, forget_t, bias, token, folds, after, heads, spans):
    rows, depth = own.shape
    groups = len(folds)
    every = gate_t.shape[0]
    width = depth + 2 * rows + LANES
    left_rows = 2 * every + 2 * heads * groups
    outs = [jax.ShapeDtypeStruct((heads, width), F32)] * groups
    outs += [jax.ShapeDtypeStruct((count, depth), BF16) for _, count in spans]
    return pl.pallas_call(
        functools.partial(local_kernel, heads, groups, spans),
        out_shape=tuple(outs),
        in_specs=[vmem()] * (6 + groups) + [pl.BlockSpec(memory_space=pl.ANY)],
        out_specs=tuple([vmem()] * len(outs)),
        scratch_shapes=[
            pltpu.VMEM((left_rows, depth), BF16),
            pltpu.VMEM((left_rows, 2 * rows), F32),
            pltpu.VMEM((groups * heads, 2 * rows), BF16),
        ],
        compiler_params=params(),
        cost_estimate=cost(2e9, 4e6),
        name="local",
    )(own, other, gate_t, forget_t, bias, token, *folds, after)


def carries(totals):
    out, running = [], jnp.zeros_like(totals[0])
    for total in reversed(totals):
        out.append(running)
        running = running + total
    return out[::-1], running


def column(stats, at):
    return stats[:, at : at + 1]


def project_kernel(heads, groups, *refs):
    message_refs = refs[:groups]
    value_ref, token_ref = refs[groups : groups + 2]
    sent_ref, kept_ref, log_ref = refs[groups + 2 : groups + 5]
    slots, left_ref = refs[groups + 5 :]
    depth = value_ref.shape[0]
    chip = lax.axis_index("tp") // 2
    for g in range(groups):
        slots[lax.rem(chip + groups - g, groups)] = message_refs[g][...]
    length = slots.shape[2] - depth - LANES
    stats = [slots[k, :, depth + length :] for k in range(groups)]
    carry, total = carries([column(s, TOTAL) for s in stats])
    peaks = [column(s, PEAK) + c for s, c in zip(stats, carry, strict=True)]
    peak = functools.reduce(jnp.maximum, peaks)
    summed = jnp.zeros((heads, depth), F32)
    denom = jnp.zeros((heads, 1), F32)
    for k in range(groups):
        scale = jnp.exp(peaks[k] - peak)
        summed = summed + scale * slots[k, :, :depth]
        denom = denom + scale * column(stats[k], DENOM)
        log_ref[:, k * length : (k + 1) * length] = slots[k, :, depth : depth + length] + carry[k]
    high, low = split2(summed)
    left_ref[...] = jnp.zeros_like(left_ref)
    left_ref[0:heads, :] = high.astype(F32)
    left_ref[heads : 2 * heads, :] = low.astype(F32)
    left_ref[2 * heads : 2 * heads + 1, :] = token_ref[...].astype(F32)
    product = jnp.dot(left_ref[...].astype(BF16), value_ref[...], preferred_element_type=F32)
    mine = message_refs[0][:, depth + length :]
    new = {at: column(mine, at) for at in (NEW_GATE, NEW_FORGET, NEW_SCORE)}
    sent_ref[:, DV:] = lane_pack(
        {TOTAL: total, PEAK: peak, DENOM: denom, CARRIED: jnp.zeros_like(total)}, heads
    )
    kept_ref[:, DV:] = lane_pack(new, heads)
    for h in range(heads):
        lanes = slice(h * DV, (h + 1) * DV)
        sent_ref[h : h + 1, :DV] = product[h : h + 1, lanes] + product[heads + h : heads + h + 1, lanes]
        kept_ref[h : h + 1, :DV] = (
            product[2 * heads : 2 * heads + 1, lanes].astype(BF16).astype(F32)
        )


def project(messages, value_weight, token, heads, rows):
    groups = len(messages)
    depth = value_weight.shape[0]
    width = messages[0].shape[1]
    left_rows = -(-(2 * heads + 1) // 16) * 16
    return pl.pallas_call(
        functools.partial(project_kernel, heads, groups),
        out_shape=(
            jax.ShapeDtypeStruct((heads, DV + LANES), F32),
            jax.ShapeDtypeStruct((heads, DV + LANES), F32),
            jax.ShapeDtypeStruct((heads, groups * 2 * rows), F32),
        ),
        in_specs=[vmem()] * (groups + 2),
        out_specs=(vmem(), vmem(), vmem()),
        scratch_shapes=[
            pltpu.VMEM((groups, heads, width), F32),
            pltpu.VMEM((left_rows, depth), F32),
        ],
        compiler_params=params(),
        cost_estimate=cost(2e9, 6e6),
        name="project",
    )(*messages, value_weight, token)


def merge(slots, mine, heads):
    radix = slots.shape[0]
    stats = [slots[k, :, DV:] for k in range(radix)]
    totals = [column(s, TOTAL) for s in stats]
    carry, total = carries(totals)
    peaks = [column(s, PEAK) + c for s, c in zip(stats, carry, strict=True)]
    peak = functools.reduce(jnp.maximum, peaks)
    numer = jnp.zeros((heads, DV), F32)
    denom = jnp.zeros((heads, 1), F32)
    after = jnp.zeros((heads, 1), F32)
    for k in range(radix):
        scale = jnp.exp(peaks[k] - peak)
        numer = numer + scale * slots[k, :, :DV]
        denom = denom + scale * column(stats[k], DENOM)
        after = after + jnp.where(mine == k, carry[k], 0.0)
    return numer, denom, total, peak, after


def place(slots, message_refs, digit):
    for k, ref in enumerate(message_refs):
        slots[digit ^ k] = ref[...]


def merge_kernel(heads, radix, stride, *refs):
    message_refs, out_ref, slots = refs[:radix], refs[radix], refs[radix + 1]
    digit = lax.rem(lax.axis_index("sp") // stride, radix)
    place(slots, message_refs, digit)
    numer, denom, total, peak, after = merge(slots, digit, heads)
    carried = message_refs[0][:, DV + CARRIED : DV + CARRIED + 1] + after
    out_ref[:, :DV] = numer
    out_ref[:, DV:] = lane_pack(
        {TOTAL: total, PEAK: peak, DENOM: denom, CARRIED: carried}, heads
    )


def finish_kernel(heads, radix, stride, *refs):
    message_refs = refs[:radix]
    kept_ref, log_ref, weight_ref, reading_ref, slots = refs[radix:]
    digit = lax.rem(lax.axis_index("sp") // stride, radix)
    place(slots, message_refs, digit)
    numer, denom, _, peak, after = merge(slots, digit, heads)
    carried = message_refs[0][:, DV + CARRIED : DV + CARRIED + 1] + after
    new = kept_ref[:, DV:]
    new_gate, new_forget = column(new, NEW_GATE), column(new, NEW_FORGET)
    stable = jnp.maximum(new_forget + peak, new_gate)
    scale = jnp.exp(new_forget + peak - stable)
    own_term = jnp.exp(new_gate - stable) * column(new, NEW_SCORE)
    numerator = numer * scale + own_term * kept_ref[:, :DV]
    denominator = denom * scale + own_term
    reading_ref[...] = numerator / jnp.maximum(jnp.abs(denominator), 1.0)
    weight_ref[...] = jnp.exp(log_ref[...] + (carried - peak))


def exchange(message, kept, log_weight, peers):
    heads, width = message.shape
    radices, left = [], peers
    while left > 1:
        radices.append(4 if left % 4 == 0 and (left // 4 == 1 or radices) else 2)
        left //= radices[-1]
    stride = 1
    for n, radix in enumerate(radices):
        others = [
            lax.ppermute(message, "sp", [(i, i ^ (k * stride)) for i in range(peers)])
            for k in range(1, radix)
        ]
        slots = [pltpu.VMEM((radix, heads, width), F32)]
        if n < len(radices) - 1:
            message = pl.pallas_call(
                functools.partial(merge_kernel, heads, radix, stride),
                out_shape=jax.ShapeDtypeStruct(message.shape, F32),
                in_specs=[vmem()] * radix,
                out_specs=vmem(),
                scratch_shapes=slots,
                compiler_params=params(4),
                cost_estimate=cost(1e6, 1e5),
                name="merge",
            )(message, *others)
        else:
            return pl.pallas_call(
                functools.partial(finish_kernel, heads, radix, stride),
                out_shape=(
                    jax.ShapeDtypeStruct(log_weight.shape, F32),
                    jax.ShapeDtypeStruct((heads, DV), F32),
                ),
                in_specs=[vmem()] * (radix + 2),
                out_specs=(vmem(), vmem()),
                scratch_shapes=slots,
                compiler_params=params(4),
                cost_estimate=cost(1e6, 1e5),
                name="finish",
            )(message, *others, kept, log_weight)
        stride *= radix


def cache_kernel(places, tile, key_tiles, aliased, *refs):
    count = len(places)
    x_refs = refs[:count]
    key_ref, value_ref = refs[count : count + 2]
    outs = refs[count + 2 + (2 if aliased else 0) :]
    key_out, value_out, token_ref, stage, sems = outs
    step, steps = pl.program_id(0), pl.num_programs(0)
    at = lax.axis_index("tp")
    groups = lax.axis_size("tp") // 2
    slot = lax.rem(step, 2)

    def copies(out, col, slot):
        made, row = [], 0
        for n, (device_rows, behind, flip, first, size) in enumerate(places):
            chip = lax.rem(at // 2 + groups - behind, groups)
            core = lax.rem(at, 2) ^ flip
            start = pl.multiple_of((chip * 2 + core) * device_rows + first, 16)
            made.append(
                pltpu.make_async_copy(
                    stage.at[slot, pl.ds(row, size), :],
                    out.at[pl.ds(start, size), pl.ds(pl.multiple_of(col, tile), tile)],
                    sems.at[slot, n],
                )
            )
            row += size
        return made

    @pl.when(step >= 2)
    def _():
        for c in copies(value_out, 0, slot):
            c.wait()

    def run(weight_ref, out, col):
        row = 0
        for x_ref in x_refs:
            size = x_ref.shape[0]
            stage[slot, row : row + size, :] = jnp.dot(
                x_ref[...], weight_ref[...], preferred_element_type=F32
            ).astype(BF16)
            row += size
        for c in copies(out, col, slot):
            c.start()

    @pl.when(step < key_tiles)
    def _():
        run(key_ref, key_out, step * tile)

    @pl.when(step >= key_tiles)
    def _():
        run(value_ref, value_out, (step - key_tiles) * tile)

    @pl.when(step == steps - 1)
    def _():
        token_ref[...] = jnp.zeros_like(token_ref)
        for c in copies(value_out, 0, slot):
            c.wait()
        for c in copies(value_out, 0, 1 - slot):
            c.wait()


def cache_rows(pieces, key_weight, value_weight, caches, shapes, tile=256):
    depth = key_weight.shape[0]
    xs = [x for x, _ in pieces]
    places = tuple(p for _, p in pieces)
    key_tiles, value_tiles = key_weight.shape[1] // tile, value_weight.shape[1] // tile
    total = sum(x.shape[0] for x in xs)
    in_specs = [pl.BlockSpec(x.shape, lambda j: (0, 0), pipeline_mode=pl.Buffered(1)) for x in xs]
    in_specs += [
        pl.BlockSpec((depth, tile), lambda j: (0, jnp.minimum(j, key_tiles - 1))),
        pl.BlockSpec((depth, tile), lambda j: (0, jnp.maximum(j - key_tiles, 0))),
    ]
    hbm = pl.BlockSpec(memory_space=pl.ANY)
    args = [*xs, key_weight, value_weight]
    aliases = {}
    if caches is not None:
        aliases = {len(args): 0, len(args) + 1: 1}
        args += list(caches)
        in_specs += [hbm, hbm]
    return pl.pallas_call(
        functools.partial(cache_kernel, places, tile, key_tiles, caches is not None),
        grid=(key_tiles + value_tiles,),
        out_shape=(
            jax.ShapeDtypeStruct(shapes[0], BF16),
            jax.ShapeDtypeStruct(shapes[1], BF16),
            jax.ShapeDtypeStruct((8, LANES), F32),
        ),
        in_specs=in_specs,
        out_specs=(hbm, hbm, pl.BlockSpec((8, LANES), lambda j: (0, 0))),
        scratch_shapes=[
            pltpu.VMEM((2, total, tile), BF16),
            pltpu.SemaphoreType.DMA((2, len(xs))),
        ],
        input_output_aliases=aliases,
        compiler_params=params(),
        cost_estimate=cost(
            2 * total * depth * (key_weight.shape[1] + value_weight.shape[1]),
            2 * depth * (key_weight.shape[1] + value_weight.shape[1]),
        ),
        name="cache",
    )(*args)


def body(
    prompt_tokens,
    key_weight,
    value_weight,
    input_weight,
    forget_weight,
    forget_bias,
    new_token,
    new_query,
):
    rows, depth = prompt_tokens.shape
    heads = key_weight.shape[1] // DQK
    devices = lax.axis_size("tp")
    chips = devices // 2
    bounds = [0, rows // 8, rows // 2, 7 * rows // 8, rows]
    spans = [(a, b - a) for a, b in zip(bounds, bounds[1:], strict=False)]

    def to_core(v):
        return lax.ppermute(v, "tp", [(i, i ^ 1) for i in range(devices)])

    def to_chip(v, ahead):
        return lax.ppermute(
            v,
            "tp",
            [(i, ((i // 2 + ahead) % chips) * 2 + i % 2) for i in range(devices)],
        )

    ahead = range(1, chips)
    query = new_query.reshape(1, -1)
    token = new_token.reshape(1, -1)
    bias = forget_bias.reshape(1, -1)
    chunks = [prompt_tokens[: spans[0][1]]]
    came = [[to_chip(chunks[0], d) for d in ahead]]
    other = to_core(prompt_tokens)
    folded, second = fold(query, key_weight, prompt_tokens, heads, *spans[1])
    folds = [folded] + [to_chip(folded, chips - d) for d in ahead]
    came.append([to_chip(second, d) for d in ahead])
    shapes = [(devices * rows, key_weight.shape[1]), (devices * rows, value_weight.shape[1])]
    weights = (key_weight, value_weight)
    *caches, done = cache_rows(
        [(prompt_tokens, (rows, 0, 0, 0, rows)), (other, (rows, 0, 1, 0, rows))],
        *weights,
        None,
        shapes,
    )
    *messages, third, fourth = local(
        prompt_tokens,
        other,
        input_weight.T,
        forget_weight.T,
        bias,
        token,
        folds,
        done,
        heads,
        spans[2:],
    )
    messages = [messages[0]] + [to_chip(messages[d], d) for d in ahead]
    came.append([to_chip(third, d) for d in ahead])
    came.append([to_chip(fourth, d) for d in ahead])
    sent, kept, log_weight = project(messages, value_weight, token, heads, rows)
    cache_weight, reading = exchange(sent, kept, log_weight, lax.axis_size("sp"))

    def pieces(which):
        out = []
        for n in which:
            for d, v in zip(ahead, came[n], strict=True):
                out.append((v, (rows, d, 0, *spans[n])))
                out.append((to_core(v), (rows, d, 1, *spans[n])))
        return out

    *caches, _ = cache_rows(pieces([0, 1]), *weights, caches, shapes)
    *caches, _ = cache_rows(pieces([2]), *weights, caches, shapes)
    *caches, _ = cache_rows(pieces([3]), *weights, caches, shapes)
    return (*caches, cache_weight, reading.reshape(-1))


def solution(mesh):
    placed = (P(("sp", "tp"), None), P(None, "tp"), P(None, "tp"), P(), P(), P(), P(), P("tp"))
    return jax.shard_map(
        body,
        mesh=mesh,
        in_specs=placed,
        out_specs=(P("sp", "tp"), P("sp", "tp"), P("tp", "sp"), P("tp")),
        check_vma=False,
    )
```

```python
import functools
import math

import jax
import jax.numpy as jnp
from jax import lax
from jax.experimental import pallas as pl
from jax.experimental.pallas import tpu as pltpu
from jax.sharding import PartitionSpec as P


DQK = 64
DV = 128
LANES = 128
F32 = jnp.float32
BF16 = jnp.bfloat16

TOTAL, PEAK, DENOM, CARRIED = 0, 1, 2, 3
NEW_GATE, NEW_FORGET, NEW_SCORE = 4, 5, 6


def params(mib=24):
    return pltpu.CompilerParams(vmem_limit_bytes=mib * 1024 * 1024)


def cost(flops, moved):
    return pl.CostEstimate(flops=int(flops), bytes_accessed=int(moved), transcendentals=0)


def vmem():
    return pl.BlockSpec(memory_space=pltpu.VMEM)


def log_sigmoid(x):
    z = jnp.exp(-jnp.abs(x))
    u = 1.0 + z
    log1p = jnp.where(u == 1.0, z, jnp.log(u) * z / jnp.where(u == 1.0, 1.0, u - 1.0))
    return jnp.minimum(x, 0.0) - log1p


def lane_pack(values, rows):
    lane = lax.broadcasted_iota(jnp.int32, (rows, LANES), 1)
    out = jnp.zeros((rows, LANES), F32)
    for at, value in values.items():
        out = jnp.where(lane == at, value, out)
    return out


def nt_dot(a, b):
    return lax.dot_general(a, b, (((1,), (1,)), ((), ())), preferred_element_type=F32)


def carries(totals):
    out, running = [], jnp.zeros_like(totals[0])
    for total in reversed(totals):
        out.append(running)
        running = running + total
    return out[::-1], running


def column(stats, at):
    return stats[:, at : at + 1]


def merge(slots, mine, heads):
    radix = slots.shape[0]
    stats = [slots[k, :, DV:] for k in range(radix)]
    totals = [column(s, TOTAL) for s in stats]
    carry, total = carries(totals)
    peaks = [column(s, PEAK) + c for s, c in zip(stats, carry, strict=True)]
    peak = functools.reduce(jnp.maximum, peaks)
    numer = jnp.zeros((heads, DV), F32)
    denom = jnp.zeros((heads, 1), F32)
    after = jnp.zeros((heads, 1), F32)
    for k in range(radix):
        scale = jnp.exp(peaks[k] - peak)
        numer = numer + scale * slots[k, :, :DV]
        denom = denom + scale * column(stats[k], DENOM)
        after = after + jnp.where(mine == k, carry[k], 0.0)
    return numer, denom, total, peak, after


def place(slots, message_refs, digit):
    for k, ref in enumerate(message_refs):
        slots[digit ^ k] = ref[...]


def merge_kernel(heads, radix, stride, *refs):
    message_refs, out_ref, slots = refs[:radix], refs[radix], refs[radix + 1]
    digit = lax.rem(lax.axis_index("sp") // stride, radix)
    place(slots, message_refs, digit)
    numer, denom, total, peak, after = merge(slots, digit, heads)
    carried = message_refs[0][:, DV + CARRIED : DV + CARRIED + 1] + after
    out_ref[:, :DV] = numer
    out_ref[:, DV:] = lane_pack(
        {TOTAL: total, PEAK: peak, DENOM: denom, CARRIED: carried}, heads
    )


def finish_kernel(heads, radix, stride, *refs):
    message_refs = refs[:radix]
    kept_ref, log_ref, weight_ref, reading_ref, slots = refs[radix:]
    digit = lax.rem(lax.axis_index("sp") // stride, radix)
    place(slots, message_refs, digit)
    numer, denom, _, peak, after = merge(slots, digit, heads)
    carried = message_refs[0][:, DV + CARRIED : DV + CARRIED + 1] + after
    new = kept_ref[:, DV:]
    new_gate, new_forget = column(new, NEW_GATE), column(new, NEW_FORGET)
    stable = jnp.maximum(new_forget + peak, new_gate)
    scale = jnp.exp(new_forget + peak - stable)
    own_term = jnp.exp(new_gate - stable) * column(new, NEW_SCORE)
    numerator = numer * scale + own_term * kept_ref[:, :DV]
    denominator = denom * scale + own_term
    reading_ref[...] = numerator / jnp.maximum(jnp.abs(denominator), 1.0)
    weight_ref[...] = jnp.exp(log_ref[...] + (carried - peak))


def to_stage(message, flip, peers):
    return lax.ppermute(message, "sp", [(i, i ^ flip) for i in range(peers)])


def exchange(message, kept, log_weight, peers):
    heads, width = message.shape
    radices, left = [], peers
    while left > 1:
        radices.append(4 if left % 4 == 0 and (left // 4 == 1 or radices) else 2)
        left //= radices[-1]
    stride = 1
    for n, radix in enumerate(radices):
        others = [to_stage(message, k * stride, peers) for k in range(1, radix)]
        slots = [pltpu.VMEM((radix, heads, width), F32)]
        if n < len(radices) - 1:
            message = pl.pallas_call(
                functools.partial(merge_kernel, heads, radix, stride),
                out_shape=jax.ShapeDtypeStruct(message.shape, F32),
                in_specs=[vmem()] * radix,
                out_specs=vmem(),
                scratch_shapes=slots,
                compiler_params=params(4),
                cost_estimate=cost(1e6, 1e5),
                name="merge",
            )(message, *others)
        else:
            return pl.pallas_call(
                functools.partial(finish_kernel, heads, radix, stride),
                out_shape=(
                    jax.ShapeDtypeStruct(log_weight.shape, F32),
                    jax.ShapeDtypeStruct((heads, DV), F32),
                ),
                in_specs=[vmem()] * (radix + 2),
                out_specs=(vmem(), vmem()),
                scratch_shapes=slots,
                compiler_params=params(4),
                cost_estimate=cost(1e6, 1e5),
                name="finish",
            )(message, *others, kept, log_weight)
        stride *= radix


def head_pick(of, first, heads, every, start):
    out = of[first : first + heads, :]
    for k in range(heads, every, heads):
        out = jnp.where(start == k, of[first + k : first + k + heads, :], out)
    return out


def own_lanes(product, top, heads):
    return jnp.concatenate(
        [product[top + h : top + h + 1, h * DV : (h + 1) * DV] for h in range(heads)], axis=0
    )


def device_of(place):
    _, behind, flip, _, _ = place
    at = lax.axis_index("tp")
    groups = lax.axis_size("tp") // 2
    return lax.rem(at // 2 + groups - behind, groups) * 2 + (lax.rem(at, 2) ^ flip)


def push(stage, outs, places, sems):
    copies, column = [], 0
    for out in outs:
        width = out.shape[1]
        top = 0
        for place in places:
            device_rows, _, _, first, size = place
            row = pl.multiple_of(device_of(place) * device_rows + first, 16)
            copies.append(
                pltpu.make_async_copy(
                    stage.at[top : top + size, column : column + width],
                    out.at[pl.ds(row, size), :],
                    sems.at[len(copies)],
                )
            )
            copies[-1].start()
            top += size
        column += width
    return copies


def rows_kernel(heads, places, kind, *refs):
    count = len(places)
    left_over = list(refs)

    def take(n=1):
        got = left_over[:n]
        del left_over[:n]
        return got

    x_refs = take(count)
    key_ref, value_ref, gate_ref, forget_ref, bias_ref, query_ref = take(6)
    (token_ref,) = take() if kind == "first" else (None,)
    earlier = list(zip(take(count), take(count), strict=True)) if kind in ("more", "last") else None
    others = list(zip(take(2), take(2), strict=True)) if kind == "last" else []
    if kind in ("next", "start", "more"):
        take(2)
    if kind == "last":
        stage, sent_ref, log_ref = take(3)
    else:
        caches = take(2)
        state_refs, weight_refs = take(count), take(count)
        (kept_ref,) = take() if kind == "first" else (None,)
        stage, sems = take(2)
    x_ref, left_ref = take(2)
    (slots,) = take() if kind == "last" else (None,)
    depth = key_ref.shape[0]
    every = gate_ref.shape[0]
    at = lax.axis_index("tp")
    start = at * heads
    tops, total = [], 0
    for ref in x_refs:
        tops.append(total)
        x_ref[total : total + ref.shape[0], :] = ref[...]
        total += ref.shape[0]
    if token_ref is not None:
        row = lax.broadcasted_iota(jnp.int32, (16, depth), 0)
        token = jnp.where(row == 0, token_ref[...].astype(F32), 0.0)
        x_ref[total : total + 16, :] = token.astype(BF16)
    keys = key_ref.shape[1]
    stage[:, :keys] = jnp.dot(x_ref[...], key_ref[...], preferred_element_type=F32).astype(BF16)
    owner = lax.broadcasted_iota(jnp.int32, (heads, keys), 1) // DQK
    head = lax.broadcasted_iota(jnp.int32, (heads, keys), 0)
    query = jnp.where(owner == head, query_ref[...].astype(F32), 0.0).astype(BF16)
    left_ref[0:every, :] = gate_ref[...]
    left_ref[every : 2 * every, :] = forget_ref[...]
    gates = nt_dot(left_ref[...], x_ref[...])
    scores = nt_dot(query, stage[:, :keys]) * (1.0 / math.sqrt(DQK))
    stage[:, keys:] = jnp.dot(x_ref[...], value_ref[...], preferred_element_type=F32).astype(BF16)
    if kind != "last":
        copies = push(stage, caches, places, sems)
    diagonal = lax.broadcasted_iota(jnp.int32, (every, every), 0) == lax.broadcasted_iota(
        jnp.int32, (every, every), 1
    )
    bias = jnp.sum(jnp.where(diagonal, bias_ref[...], 0.0), axis=1, keepdims=True)
    log_forgets = log_sigmoid(
        head_pick(gates, every, heads, every, start) + head_pick(bias, 0, heads, every, start)
    )
    input_gate = head_pick(gates, 0, heads, every, start)
    if kind == "first":
        kept_ref[:, DV:] = lane_pack(
            {
                NEW_GATE: input_gate[:, total : total + 1],
                NEW_FORGET: log_forgets[:, total : total + 1],
                NEW_SCORE: scores[:, total : total + 1],
            },
            heads,
        )
        new_value = stage[total : total + 16, keys:].astype(F32)
        kept_ref[:, :DV] = jnp.concatenate(
            [new_value[0:1, h * DV : (h + 1) * DV] for h in range(heads)], axis=0
        )
    log_forget, input_gate, scores = log_forgets[:, :total], input_gate[:, :total], scores[:, :total]

    def piece_of(axis):
        index = lax.broadcasted_iota(jnp.int32, (total, total), axis)
        return sum((index >= top).astype(jnp.int32) for top in tops[1:]) if count > 1 else 0 * index

    later = (piece_of(0) == piece_of(1)) & (
        lax.broadcasted_iota(jnp.int32, (total, total), 0)
        > lax.broadcasted_iota(jnp.int32, (total, total), 1)
    )
    later = later.astype(F32).astype(BF16)
    high = log_forget.astype(BF16)
    rest = log_forget - high.astype(F32)
    middle = rest.astype(BF16)
    low = (rest - middle.astype(F32)).astype(BF16)

    def after(v):
        return jnp.dot(v, later, preferred_element_type=F32)

    log_weight = input_gate + (after(high) + (after(middle) + after(low)))
    lane = lax.broadcasted_iota(jnp.int32, (heads, total), 1)
    within = [
        (lane >= top) & (lane < top + ref.shape[0]) for top, ref in zip(tops, x_refs, strict=True)
    ]
    floor = jnp.finfo(jnp.float32).min
    peaks = [
        jnp.max(jnp.where(m, log_weight, floor), axis=1, keepdims=True) for m in within
    ]
    totals = [jnp.sum(jnp.where(m, log_forget, 0.0), axis=1, keepdims=True) for m in within]
    peak = jnp.zeros((heads, total), F32)
    for mask, value in zip(within, peaks, strict=True):
        peak = jnp.where(mask, value, peak)
    weighted = jnp.exp(log_weight - peak) * scores
    parts = [jnp.where(m, weighted, 0.0) for m in within]
    denoms = [jnp.sum(p, axis=1, keepdims=True) for p in parts]
    product = jnp.dot(
        jnp.concatenate(parts, axis=0).astype(BF16),
        stage[0:total, keys:],
        preferred_element_type=F32,
    )
    blocks = []
    for n, (top, place) in enumerate(zip(tops, places, strict=True)):
        _, _, _, first, size = place
        numer = own_lanes(product, n * heads, heads)
        mine = log_weight[:, top : top + size]
        now = (numer, totals[n], peaks[n], denoms[n])
        if earlier is not None:
            state_ref, weight_ref = earlier[n]
            stats = state_ref[:, DV:]
            before_peak = column(stats, PEAK) + totals[n]
            both = jnp.maximum(before_peak, peaks[n])
            was, new = jnp.exp(before_peak - both), jnp.exp(peaks[n] - both)
            now = (
                was * state_ref[:, :DV] + new * numer,
                column(stats, TOTAL) + totals[n],
                both,
                was * column(stats, DENOM) + new * denoms[n],
            )
            mine = jnp.concatenate([weight_ref[:, :first] + totals[n], mine], axis=1)
        blocks.append((device_of(place), now, mine))
    if kind != "last":
        for (_, now, mine), state_ref, weight_ref in zip(
            blocks, state_refs, weight_refs, strict=True
        ):
            numer, whole, top, denom = now
            state_ref[:, :DV] = numer
            state_ref[:, DV:] = lane_pack({TOTAL: whole, PEAK: top, DENOM: denom}, heads)
            weight_ref[...] = mine
        for copy in copies:
            copy.wait()
        return
    core = lax.rem(at, 2)
    for n, (state_ref, weight_ref) in enumerate(others):
        stats = state_ref[:, DV:]
        now = (state_ref[:, :DV], *(column(stats, k) for k in (TOTAL, PEAK, DENOM)))
        blocks.append((at if n == 0 else at - core + (1 - core), now, weight_ref[...]))
    for device, (numer, whole, top, denom), _ in blocks:
        slots[device, :, :DV] = numer
        slots[device, :, DV:] = lane_pack({TOTAL: whole, PEAK: top, DENOM: denom}, heads)
    devices = slots.shape[0]
    carry, _ = carries([slots[k, :, DV + TOTAL : DV + TOTAL + 1] for k in range(devices)])
    numer, denom, whole, top, _ = merge(slots, 0, heads)
    sent_ref[:, :DV] = numer
    sent_ref[:, DV:] = lane_pack(
        {TOTAL: whole, PEAK: top, DENOM: denom, CARRIED: jnp.zeros_like(whole)}, heads
    )
    for device, _, mine in blocks:
        carried = jnp.zeros((heads, 1), F32)
        for k in range(devices):
            carried = carried + jnp.where(device == k, carry[k], 0.0)
        length = mine.shape[1]
        log_ref[:, pl.ds(pl.multiple_of(device * length, length), length)] = mine + carried


def rows_call(kind, pieces, common, heads, token=None, earlier=(), others=(), caches=None):
    key_weight, value_weight = common[:2]
    depth, keys = key_weight.shape
    values = value_weight.shape[1]
    xs = [x for x, _ in pieces]
    places = tuple(p for _, p in pieces)
    device_rows = places[0][0]
    devices = lax.axis_size("tp")
    total = sum(x.shape[0] for x in xs) + (16 if kind == "first" else 0)
    hbm = pl.BlockSpec(memory_space=pl.ANY)
    args = [*xs, *common]
    if kind == "first":
        args.append(token)
    args += [s for s, _ in earlier] + [w for _, w in earlier]
    args += [s for s, _ in others] + [w for _, w in others]
    in_specs = [vmem()] * len(args)
    aliases = {}
    if kind in ("next", "start", "more"):
        aliases = {len(args): 0, len(args) + 1: 1}
        args += list(caches)
        in_specs += [hbm, hbm]
    state = jax.ShapeDtypeStruct((heads, DV + LANES), F32)
    scratch = [
        pltpu.VMEM((total, depth), BF16),
        pltpu.VMEM((2 * common[2].shape[0], depth), BF16),
    ]
    if kind == "last":
        outs = [
            jax.ShapeDtypeStruct((total, keys + values), BF16),
            state,
            jax.ShapeDtypeStruct((heads, devices * device_rows), F32),
        ]
        out_specs = [vmem()] * 3
        scratch.append(pltpu.VMEM((devices, heads, DV + LANES), F32))
    else:
        outs = [
            jax.ShapeDtypeStruct((devices * device_rows, keys), BF16),
            jax.ShapeDtypeStruct((devices * device_rows, values), BF16),
        ]
        outs += [state] * len(xs)
        outs += [jax.ShapeDtypeStruct((heads, p[3] + p[4]), F32) for p in places]
        outs += [state] if kind == "first" else []
        out_specs = [hbm, hbm] + [vmem()] * (len(outs) - 2)
        scratch = [
            pltpu.VMEM((total, keys + values), BF16),
            pltpu.SemaphoreType.DMA((2 * len(xs),)),
            *scratch,
        ]
    return pl.pallas_call(
        functools.partial(rows_kernel, heads, places, kind),
        out_shape=tuple(outs),
        in_specs=in_specs,
        out_specs=tuple(out_specs),
        scratch_shapes=scratch,
        input_output_aliases=aliases,
        compiler_params=params(),
        cost_estimate=cost(2 * total * depth * (keys + values), 2 * depth * (keys + values)),
        name="rows",
    )(*args)


def flush_kernel(places, stage, *refs):
    *outs, sems = refs[2:]
    for copy in push(stage, outs, places, sems):
        copy.wait()


def flush(stage, places, caches):
    hbm = pl.BlockSpec(memory_space=pl.ANY)
    return pl.pallas_call(
        functools.partial(flush_kernel, places),
        out_shape=tuple(jax.ShapeDtypeStruct(c.shape, c.dtype) for c in caches),
        in_specs=[vmem(), hbm, hbm],
        out_specs=(hbm, hbm),
        scratch_shapes=[pltpu.SemaphoreType.DMA((2 * len(places),))],
        input_output_aliases={1: 0, 2: 1},
        compiler_params=params(4),
        cost_estimate=cost(1e6, 1e6),
        name="flush",
    )(stage, *caches)


def body(
    prompt_tokens,
    key_weight,
    value_weight,
    input_weight,
    forget_weight,
    forget_bias,
    new_token,
    new_query,
):
    rows, _ = prompt_tokens.shape
    heads = key_weight.shape[1] // DQK
    devices = lax.axis_size("tp")
    chips = devices // 2
    first, spans = 0, []
    for share in (2, 4, 4):
        spans.append((first, rows // share))
        first += rows // share

    def to_core(v):
        return lax.ppermute(v, "tp", [(i, i ^ 1) for i in range(devices)])

    def to_chip(v, ahead):
        return lax.ppermute(
            v,
            "tp",
            [(i, ((i // 2 + ahead) % chips) * 2 + i % 2) for i in range(devices)],
        )

    ahead = range(1, chips)
    came = [[to_chip(prompt_tokens[a : a + size], d) for d in ahead] for a, size in spans]
    other = to_core(prompt_tokens)
    common = (
        key_weight,
        value_weight,
        input_weight.T,
        forget_weight.T,
        forget_bias.reshape(1, -1),
        new_query.reshape(1, -1),
    )

    def pieces(n):
        out = []
        for d, v in zip(ahead, came[n], strict=True):
            out.append((v, (rows, d, 0, *spans[n])))
            out.append((to_core(v), (rows, d, 1, *spans[n])))
        return out

    *caches, own_state, own_weight, kept = rows_call(
        "first",
        [(prompt_tokens, (rows, 0, 0, 0, rows))],
        common,
        heads,
        token=new_token.reshape(1, -1),
    )
    *caches, other_state, other_weight = rows_call(
        "next", [(other, (rows, 0, 1, 0, rows))], common, heads, caches=caches
    )
    states = ()
    for n in range(len(spans) - 1):
        those = pieces(n)
        out = rows_call(
            "more" if n else "start", those, common, heads, earlier=states, caches=caches
        )
        caches, out = out[:2], out[2:]
        states = tuple(zip(out[: len(those)], out[len(those) :], strict=True))
    those = pieces(len(spans) - 1)
    stage, sent, log_weight = rows_call(
        "last",
        those,
        common,
        heads,
        earlier=states,
        others=((own_state, own_weight), (other_state, other_weight)),
    )
    caches = flush(stage, tuple(p for _, p in those), caches)
    cache_weight, reading = exchange(sent, kept, log_weight, lax.axis_size("sp"))
    return (*caches, cache_weight, reading.reshape(-1))


def solution(mesh):
    placed = (P(("sp", "tp"), None), P(None, "tp"), P(None, "tp"), P(), P(), P(), P(), P("tp"))

    return jax.shard_map(
        body,
        mesh=mesh,
        in_specs=placed,
        out_specs=(P("sp", "tp"), P("sp", "tp"), P("tp", "sp"), P("tp")),
        check_vma=False,
    )
```

```python
import functools
import math

import jax
import jax.numpy as jnp
from jax import lax
from jax.experimental import pallas as pl
from jax.experimental.pallas import tpu as pltpu
from jax.sharding import PartitionSpec as P


DQK = 64
DV = 128
LANES = 128
F32 = jnp.float32
BF16 = jnp.bfloat16

TOTAL, PEAK, DENOM, CARRIED = 0, 1, 2, 3
NEW_GATE, NEW_FORGET, NEW_SCORE = 4, 5, 6


def params(mib=24):
    return pltpu.CompilerParams(vmem_limit_bytes=mib * 1024 * 1024)


def cost(flops, moved):
    return pl.CostEstimate(flops=int(flops), bytes_accessed=int(moved), transcendentals=0)


def vmem():
    return pl.BlockSpec(memory_space=pltpu.VMEM)


def log_sigmoid(x):
    z = jnp.exp(-jnp.abs(x))
    u = 1.0 + z
    log1p = jnp.where(u == 1.0, z, jnp.log(u) * z / jnp.where(u == 1.0, 1.0, u - 1.0))
    return jnp.minimum(x, 0.0) - log1p


def lane_pack(values, rows):
    lane = lax.broadcasted_iota(jnp.int32, (rows, LANES), 1)
    out = jnp.zeros((rows, LANES), F32)
    for at, value in values.items():
        out = jnp.where(lane == at, value, out)
    return out


def nt_dot(a, b):
    return lax.dot_general(a, b, (((1,), (1,)), ((), ())), preferred_element_type=F32)


def carries(totals):
    out, running = [], jnp.zeros_like(totals[0])
    for total in reversed(totals):
        out.append(running)
        running = running + total
    return out[::-1], running


def column(stats, at):
    return stats[:, at : at + 1]


def merge(slots, mine, heads):
    radix = slots.shape[0]
    stats = [slots[k, :, DV:] for k in range(radix)]
    totals = [column(s, TOTAL) for s in stats]
    carry, total = carries(totals)
    peaks = [column(s, PEAK) + c for s, c in zip(stats, carry, strict=True)]
    peak = functools.reduce(jnp.maximum, peaks)
    numer = jnp.zeros((heads, DV), F32)
    denom = jnp.zeros((heads, 1), F32)
    after = jnp.zeros((heads, 1), F32)
    for k in range(radix):
        scale = jnp.exp(peaks[k] - peak)
        numer = numer + scale * slots[k, :, :DV]
        denom = denom + scale * column(stats[k], DENOM)
        after = after + jnp.where(mine == k, carry[k], 0.0)
    return numer, denom, total, peak, after


def place(slots, message_refs, digit):
    for k, ref in enumerate(message_refs):
        slots[digit ^ k] = ref[...]


def merge_kernel(heads, radix, stride, *refs):
    message_refs, out_ref, slots = refs[:radix], refs[radix], refs[radix + 1]
    digit = lax.rem(lax.axis_index("sp") // stride, radix)
    place(slots, message_refs, digit)
    numer, denom, total, peak, after = merge(slots, digit, heads)
    carried = message_refs[0][:, DV + CARRIED : DV + CARRIED + 1] + after
    out_ref[:, :DV] = numer
    out_ref[:, DV:] = lane_pack(
        {TOTAL: total, PEAK: peak, DENOM: denom, CARRIED: carried}, heads
    )


def finish_kernel(heads, radix, stride, *refs):
    message_refs = refs[:radix]
    kept_ref, log_ref, weight_ref, reading_ref, slots = refs[radix:]
    digit = lax.rem(lax.axis_index("sp") // stride, radix)
    place(slots, message_refs, digit)
    numer, denom, _, peak, after = merge(slots, digit, heads)
    carried = message_refs[0][:, DV + CARRIED : DV + CARRIED + 1] + after
    new = kept_ref[:, DV:]
    new_gate, new_forget = column(new, NEW_GATE), column(new, NEW_FORGET)
    stable = jnp.maximum(new_forget + peak, new_gate)
    scale = jnp.exp(new_forget + peak - stable)
    own_term = jnp.exp(new_gate - stable) * column(new, NEW_SCORE)
    numerator = numer * scale + own_term * kept_ref[:, :DV]
    denominator = denom * scale + own_term
    reading_ref[...] = numerator / jnp.maximum(jnp.abs(denominator), 1.0)
    weight_ref[...] = jnp.exp(log_ref[...] + (carried - peak))


def to_stage(message, flip, peers):
    return lax.ppermute(message, "sp", [(i, i ^ flip) for i in range(peers)])


def exchange(message, kept, log_weight, peers):
    heads, width = message.shape
    radices, left = [], peers
    while left > 1:
        radices.append(2 if left % 2 == 0 else left)
        left //= radices[-1]
    stride = 1
    for n, radix in enumerate(radices):
        others = [to_stage(message, k * stride, peers) for k in range(1, radix)]
        slots = [pltpu.VMEM((radix, heads, width), F32)]
        if n < len(radices) - 1:
            message = pl.pallas_call(
                functools.partial(merge_kernel, heads, radix, stride),
                out_shape=jax.ShapeDtypeStruct(message.shape, F32),
                in_specs=[vmem()] * radix,
                out_specs=vmem(),
                scratch_shapes=slots,
                compiler_params=params(4),
                cost_estimate=cost(1e6, 1e5),
                name="merge",
            )(message, *others)
        else:
            return pl.pallas_call(
                functools.partial(finish_kernel, heads, radix, stride),
                out_shape=(
                    jax.ShapeDtypeStruct(log_weight.shape, F32),
                    jax.ShapeDtypeStruct((heads, DV), F32),
                ),
                in_specs=[vmem()] * (radix + 2),
                out_specs=(vmem(), vmem()),
                scratch_shapes=slots,
                compiler_params=params(4),
                cost_estimate=cost(1e6, 1e5),
                name="finish",
            )(message, *others, kept, log_weight)
        stride *= radix


def head_pick(of, first, heads, every, start):
    out = of[first : first + heads, :]
    for k in range(heads, every, heads):
        out = jnp.where(start == k, of[first + k : first + k + heads, :], out)
    return out


def own_lanes(product, top, heads):
    return jnp.concatenate(
        [product[top + h : top + h + 1, h * DV : (h + 1) * DV] for h in range(heads)], axis=0
    )


def device_of(place):
    _, behind, flip, _, _ = place
    at = lax.axis_index("tp")
    groups = lax.axis_size("tp") // 2
    return lax.rem(at // 2 + groups - behind, groups) * 2 + (lax.rem(at, 2) ^ flip)


def push(stage, outs, places, sems):
    copies, column = [], 0
    for out in outs:
        width = out.shape[1]
        top = 0
        for place in places:
            device_rows, _, _, first, size = place
            row = pl.multiple_of(device_of(place) * device_rows + first, 16)
            copies.append(
                pltpu.make_async_copy(
                    stage.at[top : top + size, column : column + width],
                    out.at[pl.ds(row, size), :],
                    sems.at[len(copies)],
                )
            )
            copies[-1].start()
            top += size
        column += width
    return copies


def rows_kernel(heads, places, arrays, kind, *refs):
    count = len(places)
    left_over = list(refs)

    def take(n=1):
        got = left_over[:n]
        del left_over[:n]
        return got

    x_refs = take(arrays)
    key_ref, value_ref, gate_ref, forget_ref, bias_ref, query_ref = take(6)
    (token_ref,) = take() if kind == "first" else (None,)
    earlier = list(zip(take(count), take(count), strict=True)) if kind in ("more", "last") else None
    others = list(zip(take(2), take(2), strict=True)) if kind == "last" else []
    if kind in ("next", "start", "more"):
        take(2)
    if kind == "last":
        stage, sent_ref, log_ref = take(3)
    else:
        caches = take(2)
        state_refs, weight_refs = take(count), take(count)
        (kept_ref,) = take() if kind == "first" else (None,)
        stage, sems = take(2)
    x_ref, left_ref = take(2)
    (slots,) = take() if kind == "last" else (None,)
    depth = key_ref.shape[0]
    every = gate_ref.shape[0]
    at = lax.axis_index("tp")
    start = at * heads
    tops = [sum(p[4] for p in places[:n]) for n in range(count)]
    total = 0
    for ref in x_refs:
        x_ref[total : total + ref.shape[0], :] = ref[...]
        total += ref.shape[0]
    if token_ref is not None:
        row = lax.broadcasted_iota(jnp.int32, (16, depth), 0)
        token = jnp.where(row == 0, token_ref[...].astype(F32), 0.0)
        x_ref[total : total + 16, :] = token.astype(BF16)
    keys = key_ref.shape[1]
    stage[:, :keys] = jnp.dot(x_ref[...], key_ref[...], preferred_element_type=F32).astype(BF16)
    owner = lax.broadcasted_iota(jnp.int32, (heads, keys), 1) // DQK
    head = lax.broadcasted_iota(jnp.int32, (heads, keys), 0)
    query = jnp.where(owner == head, query_ref[...].astype(F32), 0.0).astype(BF16)
    left_ref[0:every, :] = gate_ref[...]
    left_ref[every : 2 * every, :] = forget_ref[...]
    gates = nt_dot(left_ref[...], x_ref[...])
    scores = nt_dot(query, stage[:, :keys]) * (1.0 / math.sqrt(DQK))
    stage[:, keys:] = jnp.dot(x_ref[...], value_ref[...], preferred_element_type=F32).astype(BF16)
    if kind != "last":
        copies = push(stage, caches, places, sems)
    diagonal = lax.broadcasted_iota(jnp.int32, (every, every), 0) == lax.broadcasted_iota(
        jnp.int32, (every, every), 1
    )
    bias = jnp.sum(jnp.where(diagonal, bias_ref[...], 0.0), axis=1, keepdims=True)
    log_forgets = log_sigmoid(
        head_pick(gates, every, heads, every, start) + head_pick(bias, 0, heads, every, start)
    )
    input_gate = head_pick(gates, 0, heads, every, start)
    if kind == "first":
        kept_ref[:, DV:] = lane_pack(
            {
                NEW_GATE: input_gate[:, total : total + 1],
                NEW_FORGET: log_forgets[:, total : total + 1],
                NEW_SCORE: scores[:, total : total + 1],
            },
            heads,
        )
        new_value = stage[total : total + 16, keys:].astype(F32)
        kept_ref[:, :DV] = jnp.concatenate(
            [new_value[0:1, h * DV : (h + 1) * DV] for h in range(heads)], axis=0
        )
    log_forget, input_gate, scores = log_forgets[:, :total], input_gate[:, :total], scores[:, :total]

    def piece_of(axis):
        index = lax.broadcasted_iota(jnp.int32, (total, total), axis)
        return sum((index >= top).astype(jnp.int32) for top in tops[1:]) if count > 1 else 0 * index

    later = (piece_of(0) == piece_of(1)) & (
        lax.broadcasted_iota(jnp.int32, (total, total), 0)
        > lax.broadcasted_iota(jnp.int32, (total, total), 1)
    )
    later = later.astype(F32).astype(BF16)
    high = log_forget.astype(BF16)
    rest = log_forget - high.astype(F32)
    middle = rest.astype(BF16)
    low = (rest - middle.astype(F32)).astype(BF16)

    def after(v):
        return jnp.dot(v, later, preferred_element_type=F32)

    log_weight = input_gate + (after(high) + (after(middle) + after(low)))
    lane = lax.broadcasted_iota(jnp.int32, (heads, total), 1)
    within = [
        (lane >= top) & (lane < top + place[4]) for top, place in zip(tops, places, strict=True)
    ]
    floor = jnp.finfo(jnp.float32).min
    peaks = [
        jnp.max(jnp.where(m, log_weight, floor), axis=1, keepdims=True) for m in within
    ]
    totals = [jnp.sum(jnp.where(m, log_forget, 0.0), axis=1, keepdims=True) for m in within]
    peak = jnp.zeros((heads, total), F32)
    for mask, value in zip(within, peaks, strict=True):
        peak = jnp.where(mask, value, peak)
    weighted = jnp.exp(log_weight - peak) * scores
    parts = [jnp.where(m, weighted, 0.0) for m in within]
    denoms = [jnp.sum(p, axis=1, keepdims=True) for p in parts]
    product = jnp.dot(
        jnp.concatenate(parts, axis=0).astype(BF16),
        stage[0:total, keys:],
        preferred_element_type=F32,
    )
    blocks = []
    for n, (top, place) in enumerate(zip(tops, places, strict=True)):
        _, _, _, first, size = place
        numer = own_lanes(product, n * heads, heads)
        mine = log_weight[:, top : top + size]
        now = (numer, totals[n], peaks[n], denoms[n])
        if earlier is not None:
            state_ref, weight_ref = earlier[n]
            stats = state_ref[:, DV:]
            before_peak = column(stats, PEAK) + totals[n]
            both = jnp.maximum(before_peak, peaks[n])
            was, new = jnp.exp(before_peak - both), jnp.exp(peaks[n] - both)
            now = (
                was * state_ref[:, :DV] + new * numer,
                column(stats, TOTAL) + totals[n],
                both,
                was * column(stats, DENOM) + new * denoms[n],
            )
            mine = jnp.concatenate([weight_ref[:, :first] + totals[n], mine], axis=1)
        blocks.append((device_of(place), now, mine))
    if kind != "last":
        for (_, now, mine), state_ref, weight_ref in zip(
            blocks, state_refs, weight_refs, strict=True
        ):
            numer, whole, top, denom = now
            state_ref[:, :DV] = numer
            state_ref[:, DV:] = lane_pack({TOTAL: whole, PEAK: top, DENOM: denom}, heads)
            weight_ref[...] = mine
        for copy in copies:
            copy.wait()
        return
    core = lax.rem(at, 2)
    for n, (state_ref, weight_ref) in enumerate(others):
        stats = state_ref[:, DV:]
        now = (state_ref[:, :DV], *(column(stats, k) for k in (TOTAL, PEAK, DENOM)))
        blocks.append((at if n == 0 else at - core + (1 - core), now, weight_ref[...]))
    for device, (numer, whole, top, denom), _ in blocks:
        slots[device, :, :DV] = numer
        slots[device, :, DV:] = lane_pack({TOTAL: whole, PEAK: top, DENOM: denom}, heads)
    devices = slots.shape[0]
    carry, _ = carries([slots[k, :, DV + TOTAL : DV + TOTAL + 1] for k in range(devices)])
    numer, denom, whole, top, _ = merge(slots, 0, heads)
    sent_ref[:, :DV] = numer
    sent_ref[:, DV:] = lane_pack(
        {TOTAL: whole, PEAK: top, DENOM: denom, CARRIED: jnp.zeros_like(whole)}, heads
    )
    for device, _, mine in blocks:
        carried = jnp.zeros((heads, 1), F32)
        for k in range(devices):
            carried = carried + jnp.where(device == k, carry[k], 0.0)
        length = mine.shape[1]
        log_ref[:, pl.ds(pl.multiple_of(device * length, length), length)] = mine + carried


def rows_call(kind, pieces, common, heads, token=None, earlier=(), others=(), caches=None):
    key_weight, value_weight = common[:2]
    depth, keys = key_weight.shape
    values = value_weight.shape[1]
    xs = [x for those, _ in pieces for x in those]
    places = tuple(p for _, p in pieces)
    device_rows = places[0][0]
    devices = lax.axis_size("tp")
    total = sum(x.shape[0] for x in xs) + (16 if kind == "first" else 0)
    hbm = pl.BlockSpec(memory_space=pl.ANY)
    args = [*xs, *common]
    if kind == "first":
        args.append(token)
    args += [s for s, _ in earlier] + [w for _, w in earlier]
    args += [s for s, _ in others] + [w for _, w in others]
    in_specs = [vmem()] * len(args)
    aliases = {}
    if kind in ("next", "start", "more"):
        aliases = {len(args): 0, len(args) + 1: 1}
        args += list(caches)
        in_specs += [hbm, hbm]
    state = jax.ShapeDtypeStruct((heads, DV + LANES), F32)
    scratch = [
        pltpu.VMEM((total, depth), BF16),
        pltpu.VMEM((2 * common[2].shape[0], depth), BF16),
    ]
    if kind == "last":
        outs = [
            jax.ShapeDtypeStruct((total, keys + values), BF16),
            state,
            jax.ShapeDtypeStruct((heads, devices * device_rows), F32),
        ]
        out_specs = [vmem()] * 3
        scratch.append(pltpu.VMEM((devices, heads, DV + LANES), F32))
    else:
        outs = [
            jax.ShapeDtypeStruct((devices * device_rows, keys), BF16),
            jax.ShapeDtypeStruct((devices * device_rows, values), BF16),
        ]
        outs += [state] * len(places)
        outs += [jax.ShapeDtypeStruct((heads, p[3] + p[4]), F32) for p in places]
        outs += [state] if kind == "first" else []
        out_specs = [hbm, hbm] + [vmem()] * (len(outs) - 2)
        scratch = [
            pltpu.VMEM((total, keys + values), BF16),
            pltpu.SemaphoreType.DMA((2 * len(places),)),
            *scratch,
        ]
    return pl.pallas_call(
        functools.partial(rows_kernel, heads, places, len(xs), kind),
        out_shape=tuple(outs),
        in_specs=in_specs,
        out_specs=tuple(out_specs),
        scratch_shapes=scratch,
        input_output_aliases=aliases,
        compiler_params=params(),
        cost_estimate=cost(2 * total * depth * (keys + values), 2 * depth * (keys + values)),
        name="rows",
    )(*args)


def cut_kernel(spans, x_ref, *refs):
    *outs, sems = refs
    copies = [
        pltpu.make_async_copy(x_ref.at[pl.ds(first, size)], out, sems.at[n])
        for n, ((first, size), out) in enumerate(zip(spans, outs, strict=True))
    ]
    for copy in copies:
        copy.start()
    for copy in copies:
        copy.wait()


def cut(x, spans):
    return pl.pallas_call(
        functools.partial(cut_kernel, spans),
        out_shape=tuple(jax.ShapeDtypeStruct((size, x.shape[1]), x.dtype) for _, size in spans),
        in_specs=[pl.BlockSpec(memory_space=pl.ANY)],
        out_specs=tuple([vmem()] * len(spans)),
        scratch_shapes=[pltpu.SemaphoreType.DMA((len(spans),))],
        compiler_params=params(4),
        cost_estimate=cost(8e9, 1e6),
        name="cut",
    )(x)


def flush_kernel(places, stage, *refs):
    *outs, sems = refs[2:]
    for copy in push(stage, outs, places, sems):
        copy.wait()


def flush(stage, places, caches):
    hbm = pl.BlockSpec(memory_space=pl.ANY)
    return pl.pallas_call(
        functools.partial(flush_kernel, places),
        out_shape=tuple(jax.ShapeDtypeStruct(c.shape, c.dtype) for c in caches),
        in_specs=[vmem(), hbm, hbm],
        out_specs=(hbm, hbm),
        scratch_shapes=[pltpu.SemaphoreType.DMA((2 * len(places),))],
        input_output_aliases={1: 0, 2: 1},
        compiler_params=params(4),
        cost_estimate=cost(1e6, 1e6),
        name="flush",
    )(stage, *caches)


UNITS = (4, 4, 4, 3, 1)
TOGETHER = ((0, 1), (2,), (3, 4))


def body(
    prompt_tokens,
    key_weight,
    value_weight,
    input_weight,
    forget_weight,
    forget_bias,
    new_token,
    new_query,
):
    rows, _ = prompt_tokens.shape
    heads = key_weight.shape[1] // DQK
    devices = lax.axis_size("tp")
    chips = devices // 2
    unit, first, spans = rows // 16, 0, []
    for units in UNITS:
        spans.append((first, units * unit))
        first += units * unit
    blocks = [(spans[w[0]][0], sum(spans[n][1] for n in w)) for w in TOGETHER]
    last = len(spans) - 1

    def to_core(v):
        return lax.ppermute(v, "tp", [(i, i ^ 1) for i in range(devices)])

    def to_chip(v, ahead, flip=0):
        return lax.ppermute(
            v,
            "tp",
            [(i, (((i // 2 + ahead) % chips) * 2 + i % 2) ^ flip) for i in range(devices)],
        )

    ahead = range(1, chips)
    chunks = [prompt_tokens[: spans[0][1]], *cut(prompt_tokens, spans[1:])]
    came = [[to_chip(v, d) for d in ahead] for v in chunks]
    crossed = [to_chip(chunks[-1], d, 1) for d in ahead]
    other = to_core(prompt_tokens)
    common = (
        key_weight,
        value_weight,
        input_weight.T,
        forget_weight.T,
        forget_bias.reshape(1, -1),
        new_query.reshape(1, -1),
    )

    def pieces(which, block):
        out = []
        for d in ahead:
            straight = [came[n][d - 1] for n in which]
            turned = [crossed[d - 1] if n == last else to_core(came[n][d - 1]) for n in which]
            out.append((straight, (rows, d, 0, *block)))
            out.append((turned, (rows, d, 1, *block)))
        return out

    *caches, own_state, own_weight, kept = rows_call(
        "first",
        [(chunks, (rows, 0, 0, 0, rows))],
        common,
        heads,
        token=new_token.reshape(1, -1),
    )
    *caches, other_state, other_weight = rows_call(
        "next", [([other], (rows, 0, 1, 0, rows))], common, heads, caches=caches
    )
    states = ()
    for n, which in enumerate(TOGETHER[:-1]):
        those = pieces(which, blocks[n])
        out = rows_call(
            "more" if n else "start", those, common, heads, earlier=states, caches=caches
        )
        caches, out = out[:2], out[2:]
        states = tuple(zip(out[: len(those)], out[len(those) :], strict=True))
    those = pieces(TOGETHER[-1], blocks[-1])
    stage, sent, log_weight = rows_call(
        "last",
        those,
        common,
        heads,
        earlier=states,
        others=((own_state, own_weight), (other_state, other_weight)),
    )
    caches = flush(stage, tuple(p for _, p in those), caches)
    cache_weight, reading = exchange(sent, kept, log_weight, lax.axis_size("sp"))
    return (*caches, cache_weight, reading.reshape(-1))


def solution(mesh):
    placed = (P(("sp", "tp"), None), P(None, "tp"), P(None, "tp"), P(), P(), P(), P(), P("tp"))

    return jax.shard_map(
        body,
        mesh=mesh,
        in_specs=placed,
        out_specs=(P("sp", "tp"), P("sp", "tp"), P("tp", "sp"), P("tp")),
        check_vma=False,
    )
```

```python
import functools
import math

import jax
import jax.numpy as jnp
from jax import lax
from jax.experimental import pallas as pl
from jax.experimental.pallas import tpu as pltpu
from jax.sharding import PartitionSpec as P


DQK = 64
DV = 128
LANES = 128
F32 = jnp.float32
BF16 = jnp.bfloat16

TOTAL, PEAK, DENOM, CARRIED = 0, 1, 2, 3
NEW_GATE, NEW_FORGET, NEW_SCORE = 4, 5, 6


def params(mib=24):
    return pltpu.CompilerParams(vmem_limit_bytes=mib * 1024 * 1024)


def cost(flops, moved):
    return pl.CostEstimate(flops=int(flops), bytes_accessed=int(moved), transcendentals=0)


def vmem():
    return pl.BlockSpec(memory_space=pltpu.VMEM)


def log_sigmoid(x):
    z = jnp.exp(-jnp.abs(x))
    u = 1.0 + z
    log1p = jnp.where(u == 1.0, z, jnp.log(u) * z / jnp.where(u == 1.0, 1.0, u - 1.0))
    return jnp.minimum(x, 0.0) - log1p


def lane_pack(values, rows):
    lane = lax.broadcasted_iota(jnp.int32, (rows, LANES), 1)
    out = jnp.zeros((rows, LANES), F32)
    for at, value in values.items():
        out = jnp.where(lane == at, value, out)
    return out


def nt_dot(a, b):
    return lax.dot_general(a, b, (((1,), (1,)), ((), ())), preferred_element_type=F32)


def carries(totals):
    out, running = [], jnp.zeros_like(totals[0])
    for total in reversed(totals):
        out.append(running)
        running = running + total
    return out[::-1], running


def column(stats, at):
    return stats[:, at : at + 1]


def merge(slots, mine, heads):
    radix = slots.shape[0]
    stats = [slots[k, :, DV:] for k in range(radix)]
    totals = [column(s, TOTAL) for s in stats]
    carry, total = carries(totals)
    peaks = [column(s, PEAK) + c for s, c in zip(stats, carry, strict=True)]
    peak = functools.reduce(jnp.maximum, peaks)
    numer = jnp.zeros((heads, DV), F32)
    denom = jnp.zeros((heads, 1), F32)
    after = jnp.zeros((heads, 1), F32)
    for k in range(radix):
        scale = jnp.exp(peaks[k] - peak)
        numer = numer + scale * slots[k, :, :DV]
        denom = denom + scale * column(stats[k], DENOM)
        after = after + jnp.where(mine == k, carry[k], 0.0)
    return numer, denom, total, peak, after


def place(slots, message_refs, digit):
    for k, ref in enumerate(message_refs):
        slots[digit ^ k] = ref[...]


def merge_kernel(heads, radix, stride, *refs):
    message_refs, out_ref, slots = refs[:radix], refs[radix], refs[radix + 1]
    digit = lax.rem(lax.axis_index("sp") // stride, radix)
    place(slots, message_refs, digit)
    numer, denom, total, peak, after = merge(slots, digit, heads)
    carried = message_refs[0][:, DV + CARRIED : DV + CARRIED + 1] + after
    out_ref[:, :DV] = numer
    out_ref[:, DV:] = lane_pack(
        {TOTAL: total, PEAK: peak, DENOM: denom, CARRIED: carried}, heads
    )


def finish_kernel(heads, radix, stride, *refs):
    message_refs = refs[:radix]
    kept_ref, log_ref, weight_ref, reading_ref, slots = refs[radix:]
    digit = lax.rem(lax.axis_index("sp") // stride, radix)
    place(slots, message_refs, digit)
    numer, denom, _, peak, after = merge(slots, digit, heads)
    carried = message_refs[0][:, DV + CARRIED : DV + CARRIED + 1] + after
    new = kept_ref[:, DV:]
    new_gate, new_forget = column(new, NEW_GATE), column(new, NEW_FORGET)
    stable = jnp.maximum(new_forget + peak, new_gate)
    scale = jnp.exp(new_forget + peak - stable)
    own_term = jnp.exp(new_gate - stable) * column(new, NEW_SCORE)
    numerator = numer * scale + own_term * kept_ref[:, :DV]
    denominator = denom * scale + own_term
    reading_ref[...] = numerator / jnp.maximum(jnp.abs(denominator), 1.0)
    weight_ref[...] = jnp.exp(log_ref[...] + (carried - peak))


def to_stage(message, flip, peers):
    return lax.ppermute(message, "sp", [(i, i ^ flip) for i in range(peers)])


def exchange(message, kept, log_weight, peers):
    heads, width = message.shape
    radices, left = [], peers
    while left > 1:
        radices.append(2 if left % 2 == 0 else left)
        left //= radices[-1]
    stride = 1
    for n, radix in enumerate(radices):
        others = [to_stage(message, k * stride, peers) for k in range(1, radix)]
        slots = [pltpu.VMEM((radix, heads, width), F32)]
        if n < len(radices) - 1:
            message = pl.pallas_call(
                functools.partial(merge_kernel, heads, radix, stride),
                out_shape=jax.ShapeDtypeStruct(message.shape, F32),
                in_specs=[vmem()] * radix,
                out_specs=vmem(),
                scratch_shapes=slots,
                compiler_params=params(4),
                cost_estimate=cost(1e6, 1e5),
                name="merge",
            )(message, *others)
        else:
            return pl.pallas_call(
                functools.partial(finish_kernel, heads, radix, stride),
                out_shape=(
                    jax.ShapeDtypeStruct(log_weight.shape, F32),
                    jax.ShapeDtypeStruct((heads, DV), F32),
                ),
                in_specs=[vmem()] * (radix + 2),
                out_specs=(vmem(), vmem()),
                scratch_shapes=slots,
                compiler_params=params(4),
                cost_estimate=cost(1e6, 1e5),
                name="finish",
            )(message, *others, kept, log_weight)
        stride *= radix


def head_pick(of, first, heads, every, start):
    out = of[first : first + heads, :]
    for k in range(heads, every, heads):
        out = jnp.where(start == k, of[first + k : first + k + heads, :], out)
    return out


def own_lanes(product, top, heads):
    return jnp.concatenate(
        [product[top + h : top + h + 1, h * DV : (h + 1) * DV] for h in range(heads)], axis=0
    )


def device_of(place):
    _, behind, flip, _, _ = place
    at = lax.axis_index("tp")
    groups = lax.axis_size("tp") // 2
    return lax.rem(at // 2 + groups - behind, groups) * 2 + (lax.rem(at, 2) ^ flip)


def push(stage, outs, places, sems):
    copies, column = [], 0
    for out in outs:
        width = out.shape[1]
        top = 0
        for place in places:
            device_rows, _, _, first, size = place
            row = pl.multiple_of(device_of(place) * device_rows + first, 16)
            copies.append(
                pltpu.make_async_copy(
                    stage.at[top : top + size, column : column + width],
                    out.at[pl.ds(row, size), :],
                    sems.at[len(copies)],
                )
            )
            copies[-1].start()
            top += size
        column += width
    return copies


def rows_kernel(heads, places, arrays, kind, *refs):
    count = len(places)
    left_over = list(refs)

    def take(n=1):
        got = left_over[:n]
        del left_over[:n]
        return got

    x_refs = take(arrays)
    key_ref, value_ref, gate_ref, forget_ref, bias_ref, query_ref = take(6)
    (token_ref,) = take() if kind == "first" else (None,)
    earlier = list(zip(take(count), take(count), strict=True)) if kind in ("more", "last") else None
    others = list(zip(take(2), take(2), strict=True)) if kind == "last" else []
    if kind in ("next", "start", "more"):
        take(2)
    if kind == "last":
        stage, sent_ref, log_ref = take(3)
    else:
        caches = take(2)
        state_refs, weight_refs = take(count), take(count)
        (kept_ref,) = take() if kind == "first" else (None,)
        stage, sems = take(2)
    x_ref, left_ref = take(2)
    (slots,) = take() if kind == "last" else (None,)
    depth = key_ref.shape[0]
    every = gate_ref.shape[0]
    at = lax.axis_index("tp")
    start = at * heads
    tops = [sum(p[4] for p in places[:n]) for n in range(count)]
    total = 0
    for ref in x_refs:
        x_ref[total : total + ref.shape[0], :] = ref[...]
        total += ref.shape[0]
    if token_ref is not None:
        row = lax.broadcasted_iota(jnp.int32, (16, depth), 0)
        token = jnp.where(row == 0, token_ref[...].astype(F32), 0.0)
        x_ref[total : total + 16, :] = token.astype(BF16)
    keys = key_ref.shape[1]
    stage[:, :keys] = jnp.dot(x_ref[...], key_ref[...], preferred_element_type=F32).astype(BF16)
    owner = lax.broadcasted_iota(jnp.int32, (heads, keys), 1) // DQK
    head = lax.broadcasted_iota(jnp.int32, (heads, keys), 0)
    query = jnp.where(owner == head, query_ref[...].astype(F32), 0.0).astype(BF16)
    left_ref[0:every, :] = gate_ref[...]
    left_ref[every : 2 * every, :] = forget_ref[...]
    gates = nt_dot(left_ref[...], x_ref[...])
    scores = nt_dot(query, stage[:, :keys]) * (1.0 / math.sqrt(DQK))
    stage[:, keys:] = jnp.dot(x_ref[...], value_ref[...], preferred_element_type=F32).astype(BF16)
    if kind != "last":
        copies = push(stage, caches, places, sems)
    diagonal = lax.broadcasted_iota(jnp.int32, (every, every), 0) == lax.broadcasted_iota(
        jnp.int32, (every, every), 1
    )
    bias = jnp.sum(jnp.where(diagonal, bias_ref[...], 0.0), axis=1, keepdims=True)
    log_forgets = log_sigmoid(
        head_pick(gates, every, heads, every, start) + head_pick(bias, 0, heads, every, start)
    )
    input_gate = head_pick(gates, 0, heads, every, start)
    if kind == "first":
        kept_ref[:, DV:] = lane_pack(
            {
                NEW_GATE: input_gate[:, total : total + 1],
                NEW_FORGET: log_forgets[:, total : total + 1],
                NEW_SCORE: scores[:, total : total + 1],
            },
            heads,
        )
        new_value = stage[total : total + 16, keys:].astype(F32)
        kept_ref[:, :DV] = jnp.concatenate(
            [new_value[0:1, h * DV : (h + 1) * DV] for h in range(heads)], axis=0
        )
    log_forget, input_gate, scores = log_forgets[:, :total], input_gate[:, :total], scores[:, :total]

    def piece_of(axis):
        index = lax.broadcasted_iota(jnp.int32, (total, total), axis)
        return sum((index >= top).astype(jnp.int32) for top in tops[1:]) if count > 1 else 0 * index

    later = (piece_of(0) == piece_of(1)) & (
        lax.broadcasted_iota(jnp.int32, (total, total), 0)
        > lax.broadcasted_iota(jnp.int32, (total, total), 1)
    )
    later = later.astype(F32).astype(BF16)
    high = log_forget.astype(BF16)
    rest = log_forget - high.astype(F32)
    middle = rest.astype(BF16)
    low = (rest - middle.astype(F32)).astype(BF16)

    def after(v):
        return jnp.dot(v, later, preferred_element_type=F32)

    log_weight = input_gate + (after(high) + (after(middle) + after(low)))
    lane = lax.broadcasted_iota(jnp.int32, (heads, total), 1)
    within = [
        (lane >= top) & (lane < top + place[4]) for top, place in zip(tops, places, strict=True)
    ]
    floor = jnp.finfo(jnp.float32).min
    peaks = [
        jnp.max(jnp.where(m, log_weight, floor), axis=1, keepdims=True) for m in within
    ]
    totals = [jnp.sum(jnp.where(m, log_forget, 0.0), axis=1, keepdims=True) for m in within]
    peak = jnp.zeros((heads, total), F32)
    for mask, value in zip(within, peaks, strict=True):
        peak = jnp.where(mask, value, peak)
    weighted = jnp.exp(log_weight - peak) * scores
    parts = [jnp.where(m, weighted, 0.0) for m in within]
    denoms = [jnp.sum(p, axis=1, keepdims=True) for p in parts]
    product = jnp.dot(
        jnp.concatenate(parts, axis=0).astype(BF16),
        stage[0:total, keys:],
        preferred_element_type=F32,
    )
    blocks = []
    for n, (top, place) in enumerate(zip(tops, places, strict=True)):
        _, _, _, first, size = place
        numer = own_lanes(product, n * heads, heads)
        mine = log_weight[:, top : top + size]
        now = (numer, totals[n], peaks[n], denoms[n])
        if earlier is not None:
            state_ref, weight_ref = earlier[n]
            stats = state_ref[:, DV:]
            before_peak = column(stats, PEAK) + totals[n]
            both = jnp.maximum(before_peak, peaks[n])
            was, new = jnp.exp(before_peak - both), jnp.exp(peaks[n] - both)
            now = (
                was * state_ref[:, :DV] + new * numer,
                column(stats, TOTAL) + totals[n],
                both,
                was * column(stats, DENOM) + new * denoms[n],
            )
            mine = jnp.concatenate([weight_ref[:, :first] + totals[n], mine], axis=1)
        blocks.append((device_of(place), now, mine))
    if kind != "last":
        for (_, now, mine), state_ref, weight_ref in zip(
            blocks, state_refs, weight_refs, strict=True
        ):
            numer, whole, top, denom = now
            state_ref[:, :DV] = numer
            state_ref[:, DV:] = lane_pack({TOTAL: whole, PEAK: top, DENOM: denom}, heads)
            weight_ref[...] = mine
        for copy in copies:
            copy.wait()
        return
    core = lax.rem(at, 2)
    for n, (state_ref, weight_ref) in enumerate(others):
        stats = state_ref[:, DV:]
        now = (state_ref[:, :DV], *(column(stats, k) for k in (TOTAL, PEAK, DENOM)))
        blocks.append((at if n == 0 else at - core + (1 - core), now, weight_ref[...]))
    for device, (numer, whole, top, denom), _ in blocks:
        slots[device, :, :DV] = numer
        slots[device, :, DV:] = lane_pack({TOTAL: whole, PEAK: top, DENOM: denom}, heads)
    devices = slots.shape[0]
    carry, _ = carries([slots[k, :, DV + TOTAL : DV + TOTAL + 1] for k in range(devices)])
    numer, denom, whole, top, _ = merge(slots, 0, heads)
    sent_ref[:, :DV] = numer
    sent_ref[:, DV:] = lane_pack(
        {TOTAL: whole, PEAK: top, DENOM: denom, CARRIED: jnp.zeros_like(whole)}, heads
    )
    for device, _, mine in blocks:
        carried = jnp.zeros((heads, 1), F32)
        for k in range(devices):
            carried = carried + jnp.where(device == k, carry[k], 0.0)
        length = mine.shape[1]
        log_ref[:, pl.ds(pl.multiple_of(device * length, length), length)] = mine + carried


def rows_call(kind, pieces, common, heads, token=None, earlier=(), others=(), caches=None):
    key_weight, value_weight = common[:2]
    depth, keys = key_weight.shape
    values = value_weight.shape[1]
    xs = [x for those, _ in pieces for x in those]
    places = tuple(p for _, p in pieces)
    device_rows = places[0][0]
    devices = lax.axis_size("tp")
    total = sum(x.shape[0] for x in xs) + (16 if kind == "first" else 0)
    hbm = pl.BlockSpec(memory_space=pl.ANY)
    args = [*xs, *common]
    if kind == "first":
        args.append(token)
    args += [s for s, _ in earlier] + [w for _, w in earlier]
    args += [s for s, _ in others] + [w for _, w in others]
    in_specs = [vmem()] * len(args)
    aliases = {}
    if kind in ("next", "start", "more"):
        aliases = {len(args): 0, len(args) + 1: 1}
        args += list(caches)
        in_specs += [hbm, hbm]
    state = jax.ShapeDtypeStruct((heads, DV + LANES), F32)
    scratch = [
        pltpu.VMEM((total, depth), BF16),
        pltpu.VMEM((2 * common[2].shape[0], depth), BF16),
    ]
    if kind == "last":
        outs = [
            jax.ShapeDtypeStruct((total, keys + values), BF16),
            state,
            jax.ShapeDtypeStruct((heads, devices * device_rows), F32),
        ]
        out_specs = [vmem()] * 3
        scratch.append(pltpu.VMEM((devices, heads, DV + LANES), F32))
    else:
        outs = [
            jax.ShapeDtypeStruct((devices * device_rows, keys), BF16),
            jax.ShapeDtypeStruct((devices * device_rows, values), BF16),
        ]
        outs += [state] * len(places)
        outs += [jax.ShapeDtypeStruct((heads, p[3] + p[4]), F32) for p in places]
        outs += [state] if kind == "first" else []
        out_specs = [hbm, hbm] + [vmem()] * (len(outs) - 2)
        scratch = [
            pltpu.VMEM((total, keys + values), BF16),
            pltpu.SemaphoreType.DMA((2 * len(places),)),
            *scratch,
        ]
    return pl.pallas_call(
        functools.partial(rows_kernel, heads, places, len(xs), kind),
        out_shape=tuple(outs),
        in_specs=in_specs,
        out_specs=tuple(out_specs),
        scratch_shapes=scratch,
        input_output_aliases=aliases,
        compiler_params=params(),
        cost_estimate=cost(2 * total * depth * (keys + values), 2 * depth * (keys + values)),
        name="rows",
    )(*args)


def cut_kernel(spans, x_ref, *refs):
    *outs, sems = refs
    copies = [
        pltpu.make_async_copy(x_ref.at[pl.ds(first, size)], out, sems.at[n])
        for n, ((first, size), out) in enumerate(zip(spans, outs, strict=True))
    ]
    for copy in copies:
        copy.start()
    for copy in copies:
        copy.wait()


def cut(x, spans):
    return pl.pallas_call(
        functools.partial(cut_kernel, spans),
        out_shape=tuple(jax.ShapeDtypeStruct((size, x.shape[1]), x.dtype) for _, size in spans),
        in_specs=[pl.BlockSpec(memory_space=pl.ANY)],
        out_specs=tuple([vmem()] * len(spans)),
        scratch_shapes=[pltpu.SemaphoreType.DMA((len(spans),))],
        compiler_params=params(4),
        cost_estimate=cost(8e9, 1e6),
        name="cut",
    )(x)


def flush_kernel(places, stage, *refs):
    *outs, sems = refs[2:]
    for copy in push(stage, outs, places, sems):
        copy.wait()


def flush(stage, places, caches):
    hbm = pl.BlockSpec(memory_space=pl.ANY)
    return pl.pallas_call(
        functools.partial(flush_kernel, places),
        out_shape=tuple(jax.ShapeDtypeStruct(c.shape, c.dtype) for c in caches),
        in_specs=[vmem(), hbm, hbm],
        out_specs=(hbm, hbm),
        scratch_shapes=[pltpu.SemaphoreType.DMA((2 * len(places),))],
        input_output_aliases={1: 0, 2: 1},
        compiler_params=params(4),
        cost_estimate=cost(1e6, 1e6),
        name="flush",
    )(stage, *caches)


UNITS = (7, 5, 3, 1)
TOGETHER = ((0,), (1,), (2, 3))


def body(
    prompt_tokens,
    key_weight,
    value_weight,
    input_weight,
    forget_weight,
    forget_bias,
    new_token,
    new_query,
):
    rows, _ = prompt_tokens.shape
    heads = key_weight.shape[1] // DQK
    devices = lax.axis_size("tp")
    chips = devices // 2
    unit, first, spans = rows // 16, 0, []
    for units in UNITS:
        spans.append((first, units * unit))
        first += units * unit
    blocks = [(spans[w[0]][0], sum(spans[n][1] for n in w)) for w in TOGETHER]
    last = len(spans) - 1

    def to_core(v):
        return lax.ppermute(v, "tp", [(i, i ^ 1) for i in range(devices)])

    def to_chip(v, ahead, flip=0):
        return lax.ppermute(
            v,
            "tp",
            [(i, (((i // 2 + ahead) % chips) * 2 + i % 2) ^ flip) for i in range(devices)],
        )

    ahead = range(1, chips)
    chunks = [prompt_tokens[a : a + size] for a, size in spans[:2]] + list(cut(prompt_tokens, spans[2:]))
    came = [[to_chip(v, d) for d in ahead] for v in chunks]
    crossed = [to_chip(chunks[-1], d, 1) for d in ahead]
    other = to_core(prompt_tokens)
    common = (
        key_weight,
        value_weight,
        input_weight.T,
        forget_weight.T,
        forget_bias.reshape(1, -1),
        new_query.reshape(1, -1),
    )

    def pieces(which, block):
        out = []
        for d in ahead:
            straight = [came[n][d - 1] for n in which]
            turned = [crossed[d - 1] if n == last else to_core(came[n][d - 1]) for n in which]
            out.append((straight, (rows, d, 0, *block)))
            out.append((turned, (rows, d, 1, *block)))
        return out

    *caches, own_state, own_weight, kept = rows_call(
        "first",
        [(chunks, (rows, 0, 0, 0, rows))],
        common,
        heads,
        token=new_token.reshape(1, -1),
    )
    *caches, other_state, other_weight = rows_call(
        "next", [([other], (rows, 0, 1, 0, rows))], common, heads, caches=caches
    )
    states = ()
    for n, which in enumerate(TOGETHER[:-1]):
        those = pieces(which, blocks[n])
        out = rows_call(
            "more" if n else "start", those, common, heads, earlier=states, caches=caches
        )
        caches, out = out[:2], out[2:]
        states = tuple(zip(out[: len(those)], out[len(those) :], strict=True))
    those = pieces(TOGETHER[-1], blocks[-1])
    stage, sent, log_weight = rows_call(
        "last",
        those,
        common,
        heads,
        earlier=states,
        others=((own_state, own_weight), (other_state, other_weight)),
    )
    caches = flush(stage, tuple(p for _, p in those), caches)
    cache_weight, reading = exchange(sent, kept, log_weight, lax.axis_size("sp"))
    return (*caches, cache_weight, reading.reshape(-1))


def solution(mesh):
    placed = (P(("sp", "tp"), None), P(None, "tp"), P(None, "tp"), P(), P(), P(), P(), P("tp"))

    return jax.shard_map(
        body,
        mesh=mesh,
        in_specs=placed,
        out_specs=(P("sp", "tp"), P("sp", "tp"), P("tp", "sp"), P("tp")),
        check_vma=False,
    )
```

```python
import functools
import math

import jax
import jax.numpy as jnp
from jax import lax
from jax.experimental import pallas as pl
from jax.experimental.pallas import tpu as pltpu
from jax.sharding import PartitionSpec as P


DQK = 64
DV = 128
LANES = 128
F32 = jnp.float32
BF16 = jnp.bfloat16

TOTAL, PEAK, DENOM, CARRIED = 0, 1, 2, 3
NEW_GATE, NEW_FORGET, NEW_SCORE = 4, 5, 6


def params(mib=24):
    return pltpu.CompilerParams(vmem_limit_bytes=mib * 1024 * 1024)


def cost(flops, moved):
    return pl.CostEstimate(flops=int(flops), bytes_accessed=int(moved), transcendentals=0)


def vmem():
    return pl.BlockSpec(memory_space=pltpu.VMEM)


def log_sigmoid(x):
    z = jnp.exp(-jnp.abs(x))
    u = 1.0 + z
    log1p = jnp.where(u == 1.0, z, jnp.log(u) * z / jnp.where(u == 1.0, 1.0, u - 1.0))
    return jnp.minimum(x, 0.0) - log1p


def lane_pack(values, rows):
    lane = lax.broadcasted_iota(jnp.int32, (rows, LANES), 1)
    out = jnp.zeros((rows, LANES), F32)
    for at, value in values.items():
        out = jnp.where(lane == at, value, out)
    return out


def nt_dot(a, b):
    return lax.dot_general(a, b, (((1,), (1,)), ((), ())), preferred_element_type=F32)


def carries(totals):
    out, running = [], jnp.zeros_like(totals[0])
    for total in reversed(totals):
        out.append(running)
        running = running + total
    return out[::-1], running


def column(stats, at):
    return stats[:, at : at + 1]


def merge(slots, mine, heads):
    radix = len(slots)
    stats = [slot[:, DV:] for slot in slots]
    totals = [column(s, TOTAL) for s in stats]
    carry, total = carries(totals)
    peaks = [column(s, PEAK) + c for s, c in zip(stats, carry, strict=True)]
    peak = functools.reduce(jnp.maximum, peaks)
    numer = jnp.zeros((heads, DV), F32)
    denom = jnp.zeros((heads, 1), F32)
    after = jnp.zeros((heads, 1), F32)
    for k in range(radix):
        scale = jnp.exp(peaks[k] - peak)
        numer = numer + scale * slots[k][:, :DV]
        denom = denom + scale * column(stats[k], DENOM)
        after = after + jnp.where(mine == k, carry[k], 0.0)
    return numer, denom, total, peak, after


def placed(message_refs, digit):
    out = []
    for at in range(len(message_refs)):
        here = message_refs[0][...]
        for k in range(1, len(message_refs)):
            here = jnp.where((digit ^ k) == at, message_refs[k][...], here)
        out.append(here)
    return out


def merge_kernel(heads, radix, stride, *refs):
    message_refs, out_ref = refs[:radix], refs[radix]
    digit = lax.rem(lax.axis_index("sp") // stride, radix)
    slots = placed(message_refs, digit)
    numer, denom, total, peak, after = merge(slots, digit, heads)
    carried = message_refs[0][:, DV + CARRIED : DV + CARRIED + 1] + after
    out_ref[:, :DV] = numer
    out_ref[:, DV:] = lane_pack(
        {TOTAL: total, PEAK: peak, DENOM: denom, CARRIED: carried}, heads
    )


def finish_kernel(heads, radix, stride, *refs):
    message_refs = refs[:radix]
    kept_ref, log_ref, weight_ref, reading_ref = refs[radix:]
    digit = lax.rem(lax.axis_index("sp") // stride, radix)
    slots = placed(message_refs, digit)
    numer, denom, _, peak, after = merge(slots, digit, heads)
    carried = message_refs[0][:, DV + CARRIED : DV + CARRIED + 1] + after
    new = kept_ref[:, DV:]
    new_gate, new_forget = column(new, NEW_GATE), column(new, NEW_FORGET)
    stable = jnp.maximum(new_forget + peak, new_gate)
    scale = jnp.exp(new_forget + peak - stable)
    own_term = jnp.exp(new_gate - stable) * column(new, NEW_SCORE)
    numerator = numer * scale + own_term * kept_ref[:, :DV]
    denominator = denom * scale + own_term
    reading_ref[...] = numerator / jnp.maximum(jnp.abs(denominator), 1.0)
    weight_ref[...] = jnp.exp(log_ref[...] + (carried - peak))


def to_stage(message, flip, peers):
    return lax.ppermute(message, "sp", [(i, i ^ flip) for i in range(peers)])


def exchange(message, kept, log_weight, peers):
    heads, _ = message.shape
    radices, left = [], peers
    while left > 1:
        radices.append(2 if left % 2 == 0 else left)
        left //= radices[-1]
    stride = 1
    for n, radix in enumerate(radices):
        others = [to_stage(message, k * stride, peers) for k in range(1, radix)]
        if n < len(radices) - 1:
            message = pl.pallas_call(
                functools.partial(merge_kernel, heads, radix, stride),
                out_shape=jax.ShapeDtypeStruct(message.shape, F32),
                in_specs=[vmem()] * radix,
                out_specs=vmem(),
                compiler_params=params(4),
                cost_estimate=cost(1e6, 1e5),
                name="merge",
            )(message, *others)
        else:
            return pl.pallas_call(
                functools.partial(finish_kernel, heads, radix, stride),
                out_shape=(
                    jax.ShapeDtypeStruct(log_weight.shape, F32),
                    jax.ShapeDtypeStruct((heads, DV), F32),
                ),
                in_specs=[vmem()] * (radix + 2),
                out_specs=(vmem(), vmem()),
                compiler_params=params(4),
                cost_estimate=cost(1e6, 1e5),
                name="finish",
            )(message, *others, kept, log_weight)
        stride *= radix


def head_pick(of, first, heads, every, start):
    out = of[first : first + heads, :]
    for k in range(heads, every, heads):
        out = jnp.where(start == k, of[first + k : first + k + heads, :], out)
    return out


def own_lanes(product, top, heads):
    return jnp.concatenate(
        [product[top + h : top + h + 1, h * DV : (h + 1) * DV] for h in range(heads)], axis=0
    )


def device_of(place):
    _, behind, flip, _, _ = place
    at = lax.axis_index("tp")
    groups = lax.axis_size("tp") // 2
    return lax.rem(at // 2 + groups - behind, groups) * 2 + (lax.rem(at, 2) ^ flip)


def push(stage, outs, places, sems):
    copies, column = [], 0
    for out in outs:
        width = out.shape[1]
        top = 0
        for place in places:
            device_rows, _, _, first, size = place
            row = pl.multiple_of(device_of(place) * device_rows + first, 16)
            copies.append(
                pltpu.make_async_copy(
                    stage.at[top : top + size, column : column + width],
                    out.at[pl.ds(row, size), :],
                    sems.at[len(copies)],
                )
            )
            copies[-1].start()
            top += size
        column += width
    return copies


def rows_kernel(heads, places, arrays, kind, *refs):
    count = len(places)
    left_over = list(refs)

    def take(n=1):
        got = left_over[:n]
        del left_over[:n]
        return got

    x_refs = take(arrays)
    key_ref, value_ref, gate_ref, forget_ref, bias_ref, query_ref = take(6)
    (token_ref,) = take() if kind == "first" else (None,)
    earlier = list(zip(take(count), take(count), strict=True)) if kind in ("more", "last") else None
    others = list(zip(take(2), take(2), strict=True)) if kind == "last" else []
    if kind in ("next", "start", "more"):
        take(2)
    if kind == "last":
        stage, sent_ref, log_ref = take(3)
    else:
        caches = take(2)
        state_refs, weight_refs = take(count), take(count)
        (kept_ref,) = take() if kind == "first" else (None,)
        stage, sems = take(2)
    x_ref, left_ref = take(2)
    (slots,) = take() if kind == "last" else (None,)
    depth = key_ref.shape[0]
    every = gate_ref.shape[0]
    at = lax.axis_index("tp")
    start = at * heads
    tops = [sum(p[4] for p in places[:n]) for n in range(count)]
    total = 0
    for ref in x_refs:
        x_ref[total : total + ref.shape[0], :] = ref[...]
        total += ref.shape[0]
    if token_ref is not None:
        row = lax.broadcasted_iota(jnp.int32, (16, depth), 0)
        token = jnp.where(row == 0, token_ref[...].astype(F32), 0.0)
        x_ref[total : total + 16, :] = token.astype(BF16)
    keys = key_ref.shape[1]
    stage[:, :keys] = jnp.dot(x_ref[...], key_ref[...], preferred_element_type=F32).astype(BF16)
    owner = lax.broadcasted_iota(jnp.int32, (heads, keys), 1) // DQK
    head = lax.broadcasted_iota(jnp.int32, (heads, keys), 0)
    query = jnp.where(owner == head, query_ref[...].astype(F32), 0.0).astype(BF16)
    left_ref[0:every, :] = gate_ref[...]
    left_ref[every : 2 * every, :] = forget_ref[...]
    gates = nt_dot(left_ref[...], x_ref[...])
    scores = nt_dot(query, stage[:, :keys]) * (1.0 / math.sqrt(DQK))
    stage[:, keys:] = jnp.dot(x_ref[...], value_ref[...], preferred_element_type=F32).astype(BF16)
    if kind != "last":
        copies = push(stage, caches, places, sems)
    diagonal = lax.broadcasted_iota(jnp.int32, (every, every), 0) == lax.broadcasted_iota(
        jnp.int32, (every, every), 1
    )
    bias = jnp.sum(jnp.where(diagonal, bias_ref[...], 0.0), axis=1, keepdims=True)
    log_forgets = log_sigmoid(
        head_pick(gates, every, heads, every, start) + head_pick(bias, 0, heads, every, start)
    )
    input_gate = head_pick(gates, 0, heads, every, start)
    if kind == "first":
        kept_ref[:, DV:] = lane_pack(
            {
                NEW_GATE: input_gate[:, total : total + 1],
                NEW_FORGET: log_forgets[:, total : total + 1],
                NEW_SCORE: scores[:, total : total + 1],
            },
            heads,
        )
        new_value = stage[total : total + 16, keys:].astype(F32)
        kept_ref[:, :DV] = jnp.concatenate(
            [new_value[0:1, h * DV : (h + 1) * DV] for h in range(heads)], axis=0
        )
    log_forget, input_gate, scores = log_forgets[:, :total], input_gate[:, :total], scores[:, :total]

    def piece_of(axis):
        index = lax.broadcasted_iota(jnp.int32, (total, total), axis)
        return sum((index >= top).astype(jnp.int32) for top in tops[1:]) if count > 1 else 0 * index

    later = (piece_of(0) == piece_of(1)) & (
        lax.broadcasted_iota(jnp.int32, (total, total), 0)
        > lax.broadcasted_iota(jnp.int32, (total, total), 1)
    )
    later = later.astype(F32).astype(BF16)
    high = log_forget.astype(BF16)
    rest = log_forget - high.astype(F32)
    middle = rest.astype(BF16)
    low = (rest - middle.astype(F32)).astype(BF16)

    def after(v):
        return jnp.dot(v, later, preferred_element_type=F32)

    log_weight = input_gate + (after(high) + (after(middle) + after(low)))
    lane = lax.broadcasted_iota(jnp.int32, (heads, total), 1)
    within = [
        (lane >= top) & (lane < top + place[4]) for top, place in zip(tops, places, strict=True)
    ]
    floor = jnp.finfo(jnp.float32).min
    peaks = [
        jnp.max(jnp.where(m, log_weight, floor), axis=1, keepdims=True) for m in within
    ]
    totals = [jnp.sum(jnp.where(m, log_forget, 0.0), axis=1, keepdims=True) for m in within]
    peak = jnp.zeros((heads, total), F32)
    for mask, value in zip(within, peaks, strict=True):
        peak = jnp.where(mask, value, peak)
    weighted = jnp.exp(log_weight - peak) * scores
    parts = [jnp.where(m, weighted, 0.0) for m in within]
    denoms = [jnp.sum(p, axis=1, keepdims=True) for p in parts]
    product = jnp.dot(
        jnp.concatenate(parts, axis=0).astype(BF16),
        stage[0:total, keys:],
        preferred_element_type=F32,
    )
    blocks = []
    for n, (top, place) in enumerate(zip(tops, places, strict=True)):
        _, _, _, first, size = place
        numer = own_lanes(product, n * heads, heads)
        mine = log_weight[:, top : top + size]
        now = (numer, totals[n], peaks[n], denoms[n])
        if earlier is not None:
            state_ref, weight_ref = earlier[n]
            stats = state_ref[:, DV:]
            before_peak = column(stats, PEAK) + totals[n]
            both = jnp.maximum(before_peak, peaks[n])
            was, new = jnp.exp(before_peak - both), jnp.exp(peaks[n] - both)
            now = (
                was * state_ref[:, :DV] + new * numer,
                column(stats, TOTAL) + totals[n],
                both,
                was * column(stats, DENOM) + new * denoms[n],
            )
            mine = jnp.concatenate([weight_ref[:, :first] + totals[n], mine], axis=1)
        blocks.append((device_of(place), now, mine))
    if kind != "last":
        for (_, now, mine), state_ref, weight_ref in zip(
            blocks, state_refs, weight_refs, strict=True
        ):
            numer, whole, top, denom = now
            state_ref[:, :DV] = numer
            state_ref[:, DV:] = lane_pack({TOTAL: whole, PEAK: top, DENOM: denom}, heads)
            weight_ref[...] = mine
        for copy in copies:
            copy.wait()
        return
    core = lax.rem(at, 2)
    for n, (state_ref, weight_ref) in enumerate(others):
        stats = state_ref[:, DV:]
        now = (state_ref[:, :DV], *(column(stats, k) for k in (TOTAL, PEAK, DENOM)))
        blocks.append((at if n == 0 else at - core + (1 - core), now, weight_ref[...]))
    for device, (numer, whole, top, denom), _ in blocks:
        slots[device, :, :DV] = numer
        slots[device, :, DV:] = lane_pack({TOTAL: whole, PEAK: top, DENOM: denom}, heads)
    devices = slots.shape[0]
    carry, _ = carries([slots[k, :, DV + TOTAL : DV + TOTAL + 1] for k in range(devices)])
    numer, denom, whole, top, _ = merge(
        [slots[k] for k in range(devices)], 0, heads
    )
    sent_ref[:, :DV] = numer
    sent_ref[:, DV:] = lane_pack(
        {TOTAL: whole, PEAK: top, DENOM: denom, CARRIED: jnp.zeros_like(whole)}, heads
    )
    for device, _, mine in blocks:
        carried = jnp.zeros((heads, 1), F32)
        for k in range(devices):
            carried = carried + jnp.where(device == k, carry[k], 0.0)
        length = mine.shape[1]
        log_ref[:, pl.ds(pl.multiple_of(device * length, length), length)] = mine + carried


def rows_call(kind, pieces, common, heads, token=None, earlier=(), others=(), caches=None):
    key_weight, value_weight = common[:2]
    depth, keys = key_weight.shape
    values = value_weight.shape[1]
    xs = [x for those, _ in pieces for x in those]
    places = tuple(p for _, p in pieces)
    device_rows = places[0][0]
    devices = lax.axis_size("tp")
    total = sum(x.shape[0] for x in xs) + (16 if kind == "first" else 0)
    hbm = pl.BlockSpec(memory_space=pl.ANY)
    args = [*xs, *common]
    if kind == "first":
        args.append(token)
    args += [s for s, _ in earlier] + [w for _, w in earlier]
    args += [s for s, _ in others] + [w for _, w in others]
    in_specs = [vmem()] * len(args)
    aliases = {}
    if kind in ("next", "start", "more"):
        aliases = {len(args): 0, len(args) + 1: 1}
        args += list(caches)
        in_specs += [hbm, hbm]
    state = jax.ShapeDtypeStruct((heads, DV + LANES), F32)
    scratch = [
        pltpu.VMEM((total, depth), BF16),
        pltpu.VMEM((2 * common[2].shape[0], depth), BF16),
    ]
    if kind == "last":
        outs = [
            jax.ShapeDtypeStruct((total, keys + values), BF16),
            state,
            jax.ShapeDtypeStruct((heads, devices * device_rows), F32),
        ]
        out_specs = [vmem()] * 3
        scratch.append(pltpu.VMEM((devices, heads, DV + LANES), F32))
    else:
        outs = [
            jax.ShapeDtypeStruct((devices * device_rows, keys), BF16),
            jax.ShapeDtypeStruct((devices * device_rows, values), BF16),
        ]
        outs += [state] * len(places)
        outs += [jax.ShapeDtypeStruct((heads, p[3] + p[4]), F32) for p in places]
        outs += [state] if kind == "first" else []
        out_specs = [hbm, hbm] + [vmem()] * (len(outs) - 2)
        scratch = [
            pltpu.VMEM((total, keys + values), BF16),
            pltpu.SemaphoreType.DMA((2 * len(places),)),
            *scratch,
        ]
    return pl.pallas_call(
        functools.partial(rows_kernel, heads, places, len(xs), kind),
        out_shape=tuple(outs),
        in_specs=in_specs,
        out_specs=tuple(out_specs),
        scratch_shapes=scratch,
        input_output_aliases=aliases,
        compiler_params=params(),
        cost_estimate=cost(2 * total * depth * (keys + values), 2 * depth * (keys + values)),
        name="rows",
    )(*args)


def cut_kernel(spans, x_ref, *refs):
    *outs, sems = refs
    copies = [
        pltpu.make_async_copy(x_ref.at[pl.ds(first, size)], out, sems.at[n])
        for n, ((first, size), out) in enumerate(zip(spans, outs, strict=True))
    ]
    for copy in copies:
        copy.start()
    for copy in copies:
        copy.wait()


def cut(x, spans):
    return pl.pallas_call(
        functools.partial(cut_kernel, spans),
        out_shape=tuple(jax.ShapeDtypeStruct((size, x.shape[1]), x.dtype) for _, size in spans),
        in_specs=[pl.BlockSpec(memory_space=pl.ANY)],
        out_specs=tuple([vmem()] * len(spans)),
        scratch_shapes=[pltpu.SemaphoreType.DMA((len(spans),))],
        compiler_params=params(4),
        cost_estimate=cost(8e9, 1e6),
        name="cut",
    )(x)


def flush_kernel(places, stage, *refs):
    *outs, sems = refs[2:]
    for copy in push(stage, outs, places, sems):
        copy.wait()


def flush(stage, places, caches):
    hbm = pl.BlockSpec(memory_space=pl.ANY)
    return pl.pallas_call(
        functools.partial(flush_kernel, places),
        out_shape=tuple(jax.ShapeDtypeStruct(c.shape, c.dtype) for c in caches),
        in_specs=[vmem(), hbm, hbm],
        out_specs=(hbm, hbm),
        scratch_shapes=[pltpu.SemaphoreType.DMA((2 * len(places),))],
        input_output_aliases={1: 0, 2: 1},
        compiler_params=params(4),
        cost_estimate=cost(1e6, 1e6),
        name="flush",
    )(stage, *caches)


UNITS = (7, 5, 3, 1)
TOGETHER = ((0,), (1,), (2, 3))


def body(
    prompt_tokens,
    key_weight,
    value_weight,
    input_weight,
    forget_weight,
    forget_bias,
    new_token,
    new_query,
):
    rows, _ = prompt_tokens.shape
    heads = key_weight.shape[1] // DQK
    devices = lax.axis_size("tp")
    chips = devices // 2
    unit, first, spans = rows // 16, 0, []
    for units in UNITS:
        spans.append((first, units * unit))
        first += units * unit
    blocks = [(spans[w[0]][0], sum(spans[n][1] for n in w)) for w in TOGETHER]
    last = len(spans) - 1

    def to_core(v):
        return lax.ppermute(v, "tp", [(i, i ^ 1) for i in range(devices)])

    def to_chip(v, ahead, flip=0):
        return lax.ppermute(
            v,
            "tp",
            [(i, (((i // 2 + ahead) % chips) * 2 + i % 2) ^ flip) for i in range(devices)],
        )

    ahead = range(1, chips)
    chunks = [prompt_tokens[a : a + size] for a, size in spans[:2]] + list(cut(prompt_tokens, spans[2:]))
    came = [[to_chip(v, d) for d in ahead] for v in chunks]
    crossed = [to_chip(chunks[-1], d, 1) for d in ahead]
    other = to_core(prompt_tokens)
    common = (
        key_weight,
        value_weight,
        input_weight.T,
        forget_weight.T,
        forget_bias.reshape(1, -1),
        new_query.reshape(1, -1),
    )

    def pieces(which, block):
        out = []
        for d in ahead:
            straight = [came[n][d - 1] for n in which]
            turned = [crossed[d - 1] if n == last else to_core(came[n][d - 1]) for n in which]
            out.append((straight, (rows, d, 0, *block)))
            out.append((turned, (rows, d, 1, *block)))
        return out

    *caches, own_state, own_weight, kept = rows_call(
        "first",
        [(chunks, (rows, 0, 0, 0, rows))],
        common,
        heads,
        token=new_token.reshape(1, -1),
    )
    *caches, other_state, other_weight = rows_call(
        "next", [([other], (rows, 0, 1, 0, rows))], common, heads, caches=caches
    )
    states = ()
    for n, which in enumerate(TOGETHER[:-1]):
        those = pieces(which, blocks[n])
        out = rows_call(
            "more" if n else "start", those, common, heads, earlier=states, caches=caches
        )
        caches, out = out[:2], out[2:]
        states = tuple(zip(out[: len(those)], out[len(those) :], strict=True))
    those = pieces(TOGETHER[-1], blocks[-1])
    stage, sent, log_weight = rows_call(
        "last",
        those,
        common,
        heads,
        earlier=states,
        others=((own_state, own_weight), (other_state, other_weight)),
    )
    caches = flush(stage, tuple(p for _, p in those), caches)
    cache_weight, reading = exchange(sent, kept, log_weight, lax.axis_size("sp"))
    return (*caches, cache_weight, reading.reshape(-1))


def solution(mesh):
    placed = (P(("sp", "tp"), None), P(None, "tp"), P(None, "tp"), P(), P(), P(), P(), P("tp"))

    return jax.shard_map(
        body,
        mesh=mesh,
        in_specs=placed,
        out_specs=(P("sp", "tp"), P("sp", "tp"), P("tp", "sp"), P("tp")),
        check_vma=False,
    )
```
